256 devices in a mesh: grp: 2 (over y), fs: 16 (over z), tp: 8 (over x, core).
Axes of the slice: x: 4, y: 2, z: 16, core: 2. Of those that a mesh axis runs over, the one named last changes fastest.
The devices are a block of a 4x16x16 slice.
Arguments:
- tokens: bfloat16 [16384, 2048], P(('grp', 'fs'), 'tp'), parts along dimension 0, may hold values from -36 to 36
- query_matrix: bfloat16 [2048, 1024], P('fs', 'tp'), may hold values from -0.125 to 0.125
- key_weight: bfloat16 [2048, 1024], P('fs', 'tp'), may hold values from -0.125 to 0.125
- value_weight: bfloat16 [2048, 2048], P('fs', 'tp'), may hold values from -0.125 to 0.125
- forget_lower_factor: bfloat16 [2048, 32], replicated, may hold values from -0.125 to 0.125
- decay_up: bfloat16 [32, 1024], replicated, may hold values from -1 to 1
- decay_bias: float32 [1024], replicated, may hold values from -1 to 8
- log_extra: float32 [16384, 1024], P(('grp', 'fs'), 'tp'), parts along dimension 0, may hold values from -0.7 to 0
- head_gain: float32 [256], replicated, may hold values from 0.1 to 1.9
- out_weight: bfloat16 [2048, 2048], P('tp', 'fs'), may hold values from -0.125 to 0.125
- mix_gain: float32 [2048], P('tp'), may hold values from 0.1 to 1.9
- up_weight: bfloat16 [2048, 8192], P('fs', 'tp'), may hold values from -0.125 to 0.125
- down_weight: bfloat16 [8192, 2048], P('tp', 'fs'), may hold values from -0.0625 to 0.0625
- out_gain: float32 [2048], P('tp'), may hold values from 0.1 to 1.9
Outputs:
- layer_out: bfloat16 [16384, 2048], P(('grp', 'fs'), 'tp'), parts along dimension 0
The draws below stay inside these ranges and needn't reach their ends.
There are 2 independent parts, one for each index of `grp`. The reference program is written for one: setup_inputs(seed, part) draws one part's arguments, and reference() takes and returns one part's arrays. A program takes and returns all parts, laid end to end along the dimension named above; an argument that names none is the same for every part. Nothing has to cross between parts.
All inputs are finite; a program needn't handle non-finite values.
Results may differ from the reference program's by a relative error of at most 0.015.
Values may be sent and summed in bfloat16 or wider, within the bound.
A program may use at most 64 MiB of HBM per device.

```python
import math
import jax
import jax.numpy as jnp
from jax import lax

D = 2048
HEADS = 8
DK = 128
DV = 256
FF = 8192
RANK = 32
SEGMENT_LENGTH = 64
SEQ = 512
OVERALL_WORDS = 8192
N_TP = 8


def draw_tokens(key, part):
    address_embeddings = jax.random.split(key, 3)
    column_index = jnp.arange(D).astype(jnp.float32)
    col_scale = 3.0 ** (column_index / (D - 1)) * jnp.exp(jax.random.uniform(address_embeddings[1], (D,), jnp.float32, 0.0, math.log(1.5))) / 1.5
    row_scale = jnp.exp(jax.random.uniform(address_embeddings[2], (OVERALL_WORDS, 1), jnp.float32, 0.0, math.log(2.0)))
    base = jnp.clip(jax.random.normal(address_embeddings[0], (OVERALL_WORDS, D), jnp.float32), -6.0, 6.0)
    return (base * col_scale * row_scale).astype(jnp.bfloat16)


def draw_decay_bias(key, part):
    address_embeddings = jax.random.split(key, 3)
    width = HEADS * DK
    picked = jax.random.randint(address_embeddings[0], (width,), 0, 2)
    fast = jax.random.uniform(address_embeddings[1], (width,), jnp.float32, -1.0, 1.5)
    slow = jax.random.uniform(address_embeddings[2], (width,), jnp.float32, 4.0, 7.0)
    return jnp.where(picked == 1, fast, slow)


def draw_log_extra(key, part):
    address_embeddings = jax.random.split(key, 3)
    width = HEADS * DK
    forget_speeds = jnp.exp(jax.random.uniform(address_embeddings[0], (OVERALL_WORDS // SEGMENT_LENGTH, width), jnp.float32, math.log(0.0005), math.log(0.004)))
    word_segments = jax.random.randint(address_embeddings[1], (OVERALL_WORDS, 1), 0, 128) == 0
    forget_intensity = jax.random.uniform(address_embeddings[2], (OVERALL_WORDS, width), jnp.float32, math.log(0.5), math.log(0.8))
    return -jnp.repeat(forget_speeds, SEGMENT_LENGTH, axis=0) + jnp.where(word_segments, forget_intensity, 0.0)


def block_levels(stream_key, dims, cuts, low, high):
    level, own = 1.0, jax.random.fold_in(stream_key, 6)
    for axis_at, shards_of in cuts:
        heights = jnp.exp(jax.random.uniform(jax.random.fold_in(own, axis_at), (shards_of,), jnp.float32, low / len(cuts), high / len(cuts)))
        level = level * jnp.repeat(heights, dims[axis_at] // shards_of).reshape([-1 if axis == axis_at else 1 for axis in range(len(dims))])
    return level


def noise(stream_key, shape, scale, bound, cuts=(), dtype=jnp.bfloat16):
    values = scale * jax.random.normal(stream_key, shape, jnp.float32)
    if cuts:
        values = values * block_levels(stream_key, shape, cuts, -0.22, 0.18)
    return jnp.clip(values, -bound, bound).astype(dtype)


def setup_inputs(seed: int = 0, part: int = 0) -> dict:
    keys = jax.random.split(jax.random.key(seed), 15)
    part_keys = jax.random.split(jax.random.fold_in(keys[14], part), 15)
    tokens = draw_tokens(jax.random.fold_in(jax.random.fold_in(keys[14], part), 71), part)
    query_matrix = noise(keys[1], (D, HEADS * DK), D ** -0.5, 0.125, ((0, 16), (1, 8)))
    key_weight = noise(keys[2], (D, HEADS * DK), D ** -0.5, 0.125, ((0, 16), (1, 8)))
    value_weight = noise(keys[3], (D, HEADS * DV), D ** -0.5, 0.125, ((0, 16), (1, 8)))
    forget_lower_factor = noise(keys[4], (D, RANK), D ** -0.5, 0.125)
    decay_up = noise(keys[5], (RANK, HEADS * DK), RANK ** -0.5, 1.0)
    decay_bias = draw_decay_bias(jax.random.fold_in(keys[14], 71), part)
    log_extra = draw_log_extra(jax.random.fold_in(jax.random.fold_in(keys[14], part), 71), part)
    head_gain = jnp.clip(1.0 + 0.18 * jax.random.normal(keys[8], (DV,), jnp.float32), 0.1, 1.9)
    out_weight = noise(keys[9], (HEADS * DV, D), (HEADS * DV) ** -0.5, 0.125, ((0, 8), (1, 16)))
    mix_gain = jnp.clip(1.0 + 0.18 * jax.random.normal(keys[10], (D,), jnp.float32), 0.1, 1.9)
    up_weight = noise(keys[11], (D, FF), D ** -0.5, 0.125, ((0, 16), (1, 8)))
    down_weight = noise(keys[12], (FF, D), FF ** -0.5, 0.0625, ((0, 8), (1, 16)))
    out_gain = jnp.clip(1.0 + 0.18 * jax.random.normal(keys[13], (D,), jnp.float32), 0.1, 1.9)
    return {"tokens": tokens, "query_matrix": query_matrix, "key_weight": key_weight, "value_weight": value_weight, "forget_lower_factor": forget_lower_factor, "decay_up": decay_up, "decay_bias": decay_bias, "log_extra": log_extra, "head_gain": head_gain, "out_weight": out_weight, "mix_gain": mix_gain, "up_weight": up_weight, "down_weight": down_weight, "out_gain": out_gain}


ALPHA = 2.0 ** 0.5
TAU = 16.0
EPS = 1e-05
HIGH = lax.Precision.HIGHEST

def block_scan(queries, key_rows, value_rows, log_decay):
    span = queries.shape[2]
    causal = (jnp.arange(span)[:, None] >= jnp.arange(span)[None, :])[:, :, None]

    def step(state, inputs):
        query_block, key_block, value_block, decay_block = inputs
        cumul = jnp.cumsum(decay_block, axis=1)
        last_cum = cumul[:, -1:, :]
        carried = jnp.einsum('hcd,hde->hce', query_block * jnp.exp(cumul), state, precision=HIGH)
        differ = cumul[:, :, None, :] - cumul[:, None, :, :]
        weights = jnp.exp(jnp.where(causal, differ, -jnp.inf))
        scores = lax.optimization_barrier(jnp.sum(query_block[:, :, None, :] * key_block[:, None, :, :] * weights, axis=-1))
        within = jnp.einsum('hij,hje->hie', scores, value_block, precision=HIGH)
        fresh = jnp.einsum('hcd,hce->hde', key_block * jnp.exp(last_cum - cumul), value_block, precision=HIGH)
        new_state = jnp.exp(last_cum[:, 0, :])[:, :, None] * state + fresh
        return (new_state, carried + within)
    start = jnp.zeros((queries.shape[1], queries.shape[3], value_rows.shape[3]), jnp.float32)
    _, outputs = lax.scan(step, start, (queries, key_rows, value_rows, log_decay))
    return outputs

def mixer_sequence(inputs):
    queries, key_rows, value_rows, log_decay = inputs
    count = queries.shape[0] // SEGMENT_LENGTH

    def blocks(array, depth):
        return array.astype(jnp.float32).reshape(count, SEGMENT_LENGTH, HEADS, depth).transpose(0, 2, 1, 3)
    outputs = block_scan(blocks(queries, DK) * DK ** (-0.5), blocks(key_rows, DK), blocks(value_rows, DV), blocks(log_decay, DK))
    return outputs.transpose(0, 2, 1, 3).reshape(queries.shape[0], HEADS, DV)

def group_sum(left, right, width):
    running = jnp.zeros((left.shape[0], right.shape[1]), jnp.float32)
    for index in range(N_TP):
        partial_sum = jnp.dot(left[:, index * width:(index + 1) * width], right[index * width:(index + 1) * width], preferred_element_type=jnp.float32).astype(jnp.bfloat16)
        partial_sum = lax.optimization_barrier(partial_sum)
        running = running + partial_sum.astype(jnp.float32)
    return running

def layer_norm(summed, gain_cols):
    row_mean = lax.optimization_barrier(jnp.mean(summed, axis=1, keepdims=True))
    centered = summed - row_mean
    row_var = lax.optimization_barrier(jnp.mean(centered * centered, axis=1, keepdims=True))
    return (centered * lax.rsqrt(row_var + EPS) * gain_cols).astype(jnp.bfloat16)

def reference(tokens, query_matrix, key_weight, value_weight, forget_lower_factor, decay_up, decay_bias, log_extra, head_gain, out_weight, mix_gain, up_weight, down_weight, out_gain):
    queries = jnp.dot(tokens, query_matrix, preferred_element_type=jnp.float32).astype(jnp.bfloat16)
    key_rows = jnp.dot(tokens, key_weight, preferred_element_type=jnp.float32).astype(jnp.bfloat16)
    value_rows = jnp.dot(tokens, value_weight, preferred_element_type=jnp.float32).astype(jnp.bfloat16)
    low = jnp.dot(tokens, forget_lower_factor, preferred_element_type=jnp.float32).astype(jnp.bfloat16)
    gate_pre = jnp.dot(low, decay_up, preferred_element_type=jnp.float32) + decay_bias
    log_decay = jax.nn.log_sigmoid(gate_pre) / TAU + log_extra
    count = tokens.shape[0] // SEQ
    attended = lax.map(mixer_sequence, (queries.reshape(count, SEQ, HEADS * DK), key_rows.reshape(count, SEQ, HEADS * DK), value_rows.reshape(count, SEQ, HEADS * DV), log_decay.reshape(count, SEQ, HEADS * DK)))
    attended = attended.reshape(tokens.shape[0], HEADS, DV)
    scaled = attended * lax.rsqrt(lax.optimization_barrier(jnp.mean(attended * attended, axis=-1, keepdims=True)) + EPS) * head_gain
    mixed_heads = scaled.reshape(tokens.shape[0], HEADS * DV).astype(jnp.bfloat16)
    mix = group_sum(mixed_heads, out_weight, HEADS * DV // N_TP)
    normed = layer_norm(ALPHA * tokens.astype(jnp.float32) + mix, mix_gain)
    hidden = jnp.dot(normed, up_weight, preferred_element_type=jnp.float32)
    activation = jnp.square(jax.nn.relu(hidden)).astype(jnp.bfloat16)
    down = group_sum(activation, down_weight, FF // N_TP)
    return layer_norm(ALPHA * normed.astype(jnp.float32) + down, out_gain)
```

```python
import functools

import jax
import jax.numpy as jnp
import numpy as np
from jax import lax
from jax.experimental import pallas as pl
from jax.experimental.pallas import tpu as pltpu
from jax.sharding import PartitionSpec as P

DK = 128
DV = 256
TILE = 128
LEVELS = (64, 32, 16, 8, 4, 2, 1)
ALPHA = 2.0**0.5
TAU = 16.0
EPS = 1e-05
MESH = pl.DeviceIdType.MESH
BF = jnp.bfloat16
F32 = jnp.float32


def decay_sums():
    i = np.arange(TILE)[:, None]
    j = np.arange(TILE)[None, :]
    parts = []
    for m in LEVELS:
        mid = i // (2 * m) * (2 * m) + m - 1
        parts.append(np.where(i > mid, (j > mid) & (j <= i), (j > i) & (j <= mid)))
    parts.append(j <= i)
    parts.append(j > i)
    one = np.concatenate(parts, axis=0).astype(np.float32)
    return np.concatenate([one, one], axis=1)


def dot(a, b, dims=((1,), (0,))):
    return lax.dot_general(a, b, (dims, ((), ())), preferred_element_type=F32)


NT = ((1,), (1,))
TN = ((0,), (0,))


def kernel(
    n_fs,
    n_tp,
    tokens,
    q_w,
    k_w,
    v_w,
    o_w,
    up_w,
    dn_w,
    fl,
    d_up,
    d_bias,
    extra,
    h_gain,
    m_gain,
    o_gain,
    sums,
    out,
    tok,
    wqkv,
    wo,
    wup,
    wdn,
    esum,
    mixed,
    part1,
    part2,
    half_recv,
    fwd_recv,
    last_recv,
    fwd_send,
    last_send,
    nrm,
    act,
    own_out,
    out_buf,
    mg_all,
    og_all,
    local_sem,
    z_send,
    z_recv,
    y_send,
    y_recv,
    ag_send,
    ag_recv,
    rs_send,
    rs_recv,
    small_send,
    small_recv,
):
    z = lax.axis_index("fs")
    t = lax.axis_index("tp")
    grp = lax.axis_index("grp")
    g = lax.rem(grp, 2)
    mate = grp + 1 - 2 * g
    n_x = n_tp // 2
    x, c = t // 2, lax.rem(t, 2)
    right_t = 2 * lax.rem(x + 1, n_x) + c
    left_t = 2 * lax.rem(x + n_x - 1, n_x) + c
    across_t = 2 * lax.rem(x + 2, n_x) + c
    twin_t = t + 1 - 2 * c
    right_z = lax.rem(z + 1, n_fs)
    left_z = lax.rem(z + n_fs - 1, n_fs)
    rows = tok.shape[0]
    cols = tokens.shape[1]
    width = tok.shape[1]
    block = rows // n_tp
    zd = q_w.shape[0]

    def at(v, step):
        return pl.multiple_of(v * step, step)

    def remote(src, dst, ssem, rsem, dev):
        return pltpu.make_async_remote_copy(
            src_ref=src,
            dst_ref=dst,
            send_sem=ssem,
            recv_sem=rsem,
            device_id=dev,
            device_id_type=MESH,
        )

    pending = []

    def send(src, dst, ssem, rsem, dev):
        copy = remote(src, dst, ssem, rsem, dev)
        copy.start()
        pending.append(copy)

    def arrive(dst, ssem, rsem, dev):
        remote(dst, dst, ssem, rsem, dev).wait_recv()

    my_cols = pl.ds(at(z, zd), zd)
    kw = q_w.shape[1]
    vw = v_w.shape[1]
    own_rows = pl.ds(at(z, zd), zd)
    moves = [
        (q_w, wqkv.at[own_rows, pl.ds(0, kw)]),
        (k_w, wqkv.at[own_rows, pl.ds(kw, kw)]),
        (v_w, wqkv.at[own_rows, pl.ds(2 * kw, vw)]),
        (tokens, tok.at[:, pl.ds(at(t, cols), cols)]),
        (o_w, wo.at[:, my_cols]),
        (up_w, wup.at[own_rows, :]),
        (dn_w, wdn.at[:, my_cols]),
    ]
    moves = [pltpu.make_async_copy(s, d, local_sem.at[i]) for i, (s, d) in enumerate(moves)]
    for m in moves:
        m.start()

    barrier = pltpu.get_barrier_semaphore()
    peers = [{"fs": left_z}, {"fs": right_z}, {"grp": mate}]
    peers += [{"tp": lax.rem(t + k, n_tp)} for k in range(1, n_tp)]
    for p in peers:
        pl.semaphore_signal(barrier, inc=1, device_id=p, device_id_type=MESH)
    pl.semaphore_wait(barrier, len(peers))

    hq = zd // 2
    hu = zd // 4
    ho = wo.shape[0] // 2
    hd = wdn.shape[0] // 4

    def region(p, s, which):
        c0 = pl.ds(at(s, zd), zd)
        if p == 0:
            return wqkv.at[pl.ds(pl.multiple_of(s * zd + which * hq, hq), hq), :]
        if p == 1:
            return wo.at[pl.ds(at(which, ho), ho), c0]
        if p == 2:
            return wup.at[pl.ds(pl.multiple_of(s * zd + which * hu, hu), hu), :]
        if p == 3:
            return wdn.at[pl.ds(at(which, hd), hd), c0]
        if p in (4, 5):
            return wup.at[pl.ds(pl.multiple_of(s * zd + (p - 2) * hu, hu), hu), :]
        return wdn.at[pl.ds((p - 4) * hd, hd), c0]

    def whole(p):
        n = n_fs - 1
        if p == 0:
            return wqkv.at[pl.ds(0, n * hq), :]
        if p == 1:
            return wo.at[pl.ds(0, ho), pl.ds(0, n * zd)]
        if p in (2, 4, 5):
            return wup.at[pl.ds(0, n * hu), :]
        return wdn.at[pl.ds(0, hd), pl.ds(0, n * zd)]

    far = n_fs // 2
    near = n_fs - 1 - far
    reach = [(far, near) if p in (0, 2, 4, 6) else (near, far) for p in range(8)]

    def origin(d, h):
        return lax.rem(z + (n_fs - h if d == 0 else h), n_fs)

    def z_start(p, d, h):
        dev = {"fs": right_z if d == 0 else left_z}
        r = region(p, z if h == 1 else origin(d, h - 1), g)
        remote(r, r, z_send.at[p], z_recv.at[p, d, h - 1], dev).start()

    def z_event(p, d, h):
        dev = {"fs": left_z if d == 0 else right_z}
        arrive(region(p, origin(d, h), g), z_send.at[p], z_recv.at[p, d, h - 1], dev)
        if h < reach[p][d]:
            z_start(p, d, h + 1)

    def y_slot(d, h):
        return d * far + h - 1

    def y_start(p, d, h):
        r = region(p, origin(d, h), g)
        remote(r, r, y_send.at[p], y_recv.at[p, y_slot(d, h)], {"grp": mate}).start()

    def y_done(p):
        for d in range(2):
            for h in range(1, reach[p][d] + 1):
                r = region(p, origin(d, h), 1 - g)
                arrive(r, y_send.at[p], y_recv.at[p, y_slot(d, h)], {"grp": mate})

    first, second = (0, 1, 2), (3, 4, 6, 5, 7)
    order = []
    for h in range(1, far + 1):
        for p in first:
            for d in range(2):
                if h <= reach[p][d]:
                    order.append(functools.partial(z_event, p, d, h))
                    if p == 0:
                        order.append(functools.partial(y_start, p, d, h))
        if h == far - 1:
            for p in second:
                for d in range(2):
                    order.append(functools.partial(z_start, p, d, 1))
    split = len(order)
    for p in (1, 2):
        for h in range(1, far + 1):
            for d in range(2):
                if h <= reach[p][d]:
                    order.append(functools.partial(y_start, p, d, h))
    tail_from = len(order)
    for h in range(1, far + 1):
        for p in second:
            for d in range(2):
                if h <= reach[p][d]:
                    order.append(functools.partial(z_event, p, d, h))
                    if p == 3:
                        order.append(functools.partial(y_start, p, d, h))
    done = [0]

    def pump(upto):
        while done[0] < min(upto, len(order)):
            order[done[0]]()
            done[0] += 1

    def ease(n):
        pump(done[0] + n)

    def gather(i, view):
        ss, rs = ag_send.at[i], ag_recv.at[i]
        right, left, twin = {"tp": right_t}, {"tp": left_t}, {"tp": twin_t}

        def go(k, blk, half, dev):
            v = view(blk, half)
            send(v, v, ss.at[k], rs.at[k], dev)

        def got(k, blk, half, dev):
            arrive(view(blk, half), ss.at[k], rs.at[k], dev)

        def start():
            go(0, t, None, right)
            go(1, t, None, left)
            go(2, t, None, twin)

        def middle():
            got(0, left_t, None, left)
            go(3, left_t, 0, right)
            go(4, left_t, None, twin)
            got(1, right_t, None, right)
            go(5, right_t, 1, left)
            go(6, right_t, None, twin)

        def close():
            got(3, across_t, 0, left)
            go(7, across_t, 0, twin)
            got(5, across_t, 1, right)
            go(8, across_t, 1, twin)

        def finish():
            flip = 1 - 2 * c
            got(2, twin_t, None, twin)
            got(4, left_t + flip, None, twin)
            got(6, right_t + flip, None, twin)
            got(7, across_t + flip, 0, twin)
            got(8, across_t + flip, 1, twin)

        return start, middle, close, finish

    def tok_view(blk, half):
        r = pl.ds(0, rows) if half is None else pl.ds(half * (rows // 2), rows // 2)
        return tok.at[r, pl.ds(at(blk, cols), cols)]

    def nrm_view(blk, half):
        cc = pl.ds(0, width) if half is None else pl.ds(half * (width // 2), width // 2)
        return nrm.at[pl.ds(at(blk, block), block), cc]

    def scatter_sum(i, part):
        ss, rs = rs_send.at[i], rs_recv.at[i]
        right, left, twin = {"tp": right_t}, {"tp": left_t}, {"tp": twin_t}
        hw = width // 2

        for k in (2, 1, 3, 0):
            xx = lax.rem(x + k, n_x)
            send(
                part.at[pl.ds(at(2 * xx + 1 - c, block), block), :],
                half_recv.at[i, k],
                ss.at[k],
                rs.at[k],
                twin,
            )

        def pair(k):
            arrive(half_recv.at[i, k], ss.at[k], rs.at[k], twin)
            xx = lax.rem(x + k, n_x)
            mine = part[pl.ds(at(2 * xx + c, block), block), :]
            return mine.astype(F32) + half_recv[i, k].astype(F32)

        fwd_send[i] = pair(2).astype(BF)
        for k, (lo, dev) in enumerate(((0, right), (hw, left))):
            send(
                fwd_send.at[i, :, pl.ds(lo, hw)],
                fwd_recv.at[i, k],
                ss.at[4 + k],
                rs.at[4 + k],
                dev,
            )
        s1, s3 = pair(1), pair(3)
        last_send[i, 0, :, pl.ds(hw, hw)] = s1[:, hw:].astype(BF)
        last_send[i, 1, :, pl.ds(0, hw)] = s3[:, :hw].astype(BF)
        yield
        arrive(fwd_recv.at[i, 0], ss.at[4], rs.at[4], left)
        last_send[i, 0, :, pl.ds(0, hw)] = (s1[:, :hw] + fwd_recv[i, 0].astype(F32)).astype(BF)
        send(last_send.at[i, 0], last_recv.at[i, 0], ss.at[6], rs.at[6], right)
        arrive(fwd_recv.at[i, 1], ss.at[5], rs.at[5], right)
        last_send[i, 1, :, pl.ds(hw, hw)] = (s3[:, hw:] + fwd_recv[i, 1].astype(F32)).astype(BF)
        send(last_send.at[i, 1], last_recv.at[i, 1], ss.at[7], rs.at[7], left)
        total = pair(0)
        yield
        arrive(last_recv.at[i, 0], ss.at[6], rs.at[6], left)
        arrive(last_recv.at[i, 1], ss.at[7], rs.at[7], right)
        yield total + last_recv[i, 0].astype(F32) + last_recv[i, 1].astype(F32)

    def norm(v, gain):
        mean = jnp.mean(v, axis=1, keepdims=True)
        d = v - mean
        var = jnp.mean(d * d, axis=1, keepdims=True)
        return (d * lax.rsqrt(var + EPS) * gain).astype(BF)

    for i in (0, 1, 2):
        moves[i].wait()
    for d in range(2):
        z_start(0, d, 1)
    moves[3].wait()
    tok_start, tok_middle, tok_close, tok_finish = gather(0, tok_view)
    tok_start()
    for i in (4, 5, 6):
        moves[i].wait()
    for p in (1, 2):
        for d in range(2):
            z_start(p, d, 1)
    mine = pl.ds(at(t, cols), cols)
    for j, (src, dst) in enumerate(((m_gain, mg_all), (o_gain, og_all))):
        dst[:, mine] = src[...]
        for k in range(1, n_tp):
            send(
                src,
                dst.at[:, mine],
                small_send.at[j, k],
                small_recv.at[j, k],
                {"tp": lax.rem(t + k, n_tp)},
            )

    per_hop = 8
    pump(2 * per_hop)
    tok_middle()
    pump(3 * per_hop)
    tok_close()
    pump(4 * per_hop)
    tok_finish()

    key_cols = pl.ds(at(t, DK), DK)
    n_tiles = rows // TILE
    for i in range(n_tiles):
        rr = pl.ds(i * TILE, TILE)
        low = dot(tok[rr, :], fl[...]).astype(BF)
        pre = dot(low, d_up[:, key_cols]) + d_bias[:, key_cols]
        log_sig = jnp.minimum(pre, 0.0) - jnp.log1p(jnp.exp(-jnp.abs(pre)))
        decay = log_sig / TAU + extra[rr, :]
        hi = decay.astype(BF)
        lo = (decay - hi.astype(F32)).astype(BF)
        esum[i] = jnp.exp(dot(sums[...], jnp.concatenate([hi, lo], axis=0)))
        pump((5 + i) * per_hop)
    pump(tail_from)
    y_done(0)

    ii = lax.broadcasted_iota(jnp.int32, (TILE, TILE), 0)
    jj = lax.broadcasted_iota(jnp.int32, (TILE, TILE), 1)
    state = jnp.zeros((DV, DK), F32)
    n_lv = len(LEVELS)
    for i in range(n_tiles):
        rr = pl.ds(i * TILE, TILE)
        qkv = dot(tok[rr, :], wqkv[...]).astype(BF)
        ease(4)
        q = qkv[:, :DK].astype(F32) * DK**-0.5
        kb = qkv[:, DK : 2 * DK]
        k = kb.astype(F32)
        v = qkv[:, 2 * DK :]
        scores = jnp.where(ii == jj, dot(q.astype(BF), kb, NT), 0.0)
        for l, m in enumerate(LEVELS):
            e = esum[i, pl.ds(l * TILE, TILE), :]
            s = dot((q * e).astype(BF), (k * e).astype(BF), NT)
            scores = jnp.where(((ii ^ jj) // m == 1) & (ii > jj), s, scores)
        e_in = esum[i, pl.ds(n_lv * TILE, TILE), :]
        e_out = esum[i, pl.ds((n_lv + 1) * TILE, TILE), :]
        got = dot(scores.astype(BF), v)
        if i > 0:
            got = got + dot((q * e_in).astype(BF), state.astype(BF), NT)
        if i < n_tiles - 1:
            fresh = dot(v, (k * e_out).astype(BF), TN)
            state = state * e_in[TILE - 1 : TILE, :] + fresh
        scale = lax.rsqrt(jnp.mean(got * got, axis=1, keepdims=True) + EPS)
        mixed[rr, :] = (got * scale * h_gain[...]).astype(BF)
        ease(2)
    y_done(1)

    step = 256

    def mix_cols(j, _):
        cc = pl.ds(pl.multiple_of(j * step, step), step)
        part1[:, cc] = dot(mixed[...], wo[:, cc]).astype(BF)
        return 0

    lax.fori_loop(0, width // step, mix_cols, 0)
    rs1 = scatter_sum(0, part1)
    next(rs1)
    ease(6)
    next(rs1)
    ease(10)
    mix = next(rs1)
    for j, dst in enumerate((mg_all, og_all)):
        for k in range(1, n_tp):
            src_t = lax.rem(t + n_tp - k, n_tp)
            arrive(
                dst.at[:, pl.ds(at(src_t, cols), cols)],
                small_send.at[j, k],
                small_recv.at[j, k],
                {"tp": src_t},
            )
    my_rows = pl.ds(at(t, block), block)
    nrm[my_rows, :] = norm(ALPHA * tok[my_rows, :].astype(F32) + mix, mg_all[...])
    n_start, n_middle, n_close, n_finish = gather(1, nrm_view)
    n_start()
    ease(10)
    n_middle()
    ease(6)
    n_close()
    n_finish()
    pump(len(order))
    y_done(2)

    def up_cols(j, _):
        cc = pl.ds(pl.multiple_of(j * step, step), step)
        hidden = jnp.maximum(dot(nrm[...], wup[:, cc]), 0.0)
        act[:, cc] = (hidden * hidden).astype(BF)
        return 0

    lax.fori_loop(0, act.shape[1] // step, up_cols, 0)
    y_done(3)

    def down_cols(j, _):
        cc = pl.ds(pl.multiple_of(j * step, step), step)
        part2[:, cc] = dot(act[...], wdn[:, cc]).astype(BF)
        return 0

    lax.fori_loop(0, width // step, down_cols, 0)
    rs2 = scatter_sum(1, part2)
    next(rs2)
    next(rs2)
    down = next(rs2)
    own_out[...] = norm(ALPHA * nrm[my_rows, :].astype(F32) + down, og_all[...])
    out_buf[my_rows, :] = own_out[:, mine]
    for k in range(1, n_tp):
        dst_t = lax.rem(t + k, n_tp)
        send(
            own_out.at[:, pl.ds(at(dst_t, cols), cols)],
            out_buf.at[my_rows, :],
            small_send.at[2, k],
            small_recv.at[2, k],
            {"tp": dst_t},
        )
    for k in range(1, n_tp):
        src_t = lax.rem(t + n_tp - k, n_tp)
        arrive(
            out_buf.at[pl.ds(at(src_t, block), block), :],
            small_send.at[2, k],
            small_recv.at[2, k],
            {"tp": src_t},
        )
    out[...] = out_buf[...]
    for copy in pending:
        copy.wait_send()
    for p in range(8):
        w = whole(p)
        remote(w, w, z_send.at[p], z_recv.at[p, 0, 0], {"fs": right_z}).wait_send()
        if p < 4:
            remote(w, w, y_send.at[p], y_recv.at[p, 0], {"grp": mate}).wait_send()


def solution(mesh):
    n_fs, n_tp = mesh.shape["fs"], mesh.shape["tp"]
    assert n_tp == 8 and mesh.shape["grp"] % 2 == 0

    def local(
        tokens,
        query_matrix,
        key_weight,
        value_weight,
        forget_lower_factor,
        decay_up,
        decay_bias,
        log_extra,
        head_gain,
        out_weight,
        mix_gain,
        up_weight,
        down_weight,
        out_gain,
    ):
        rows, cols = tokens.shape
        width = cols * n_tp
        block = rows // n_tp
        zd = query_matrix.shape[0]
        hidden = up_weight.shape[1]
        vcols = value_weight.shape[1]
        qkv_cols = 2 * query_matrix.shape[1] + vcols
        sums = jnp.asarray(decay_sums(), BF)
        hbm = pl.BlockSpec(memory_space=pl.ANY)
        vmem = pl.BlockSpec(memory_space=pltpu.VMEM)
        far = n_fs // 2
        dma = pltpu.SemaphoreType.DMA
        return pl.pallas_call(
            functools.partial(kernel, n_fs, n_tp),
            out_shape=jax.ShapeDtypeStruct((rows, cols), BF),
            in_specs=[hbm] * 7 + [vmem] * 8,
            out_specs=vmem,
            scratch_shapes=[
                pltpu.VMEM((rows, width), BF),
                pltpu.VMEM((width, qkv_cols), BF),
                pltpu.VMEM((vcols, width), BF),
                pltpu.VMEM((width, hidden), BF),
                pltpu.VMEM((hidden, width), BF),
                pltpu.VMEM((rows // TILE, sums.shape[0], DK), F32),
                pltpu.VMEM((rows, vcols), BF),
                pltpu.VMEM((rows, width), BF),
                pltpu.VMEM((rows, width), BF),
                pltpu.VMEM((2, n_tp // 2, block, width), BF),
                pltpu.VMEM((2, 2, block, width // 2), BF),
                pltpu.VMEM((2, 2, block, width), BF),
                pltpu.VMEM((2, block, width), BF),
                pltpu.VMEM((2, 2, block, width), BF),
                pltpu.VMEM((rows, width), BF),
                pltpu.VMEM((rows, hidden), BF),
                pltpu.VMEM((block, width), BF),
                pltpu.VMEM((rows, cols), BF),
                pltpu.VMEM((1, width), F32),
                pltpu.VMEM((1, width), F32),
                dma((7,)),
                dma((8,)),
                dma((8, 2, far)),
                dma((4,)),
                dma((4, n_fs)),
                dma((2, 9)),
                dma((2, 9)),
                dma((2, 8)),
                dma((2, 8)),
                dma((3, n_tp)),
                dma((3, n_tp)),
            ],
            compiler_params=pltpu.CompilerParams(
                collective_id=0,
                has_side_effects=True,
                vmem_limit_bytes=60 * 1024 * 1024,
            ),
            name="layer",
        )(
            tokens,
            query_matrix,
            key_weight,
            value_weight,
            out_weight,
            up_weight,
            down_weight,
            forget_lower_factor,
            decay_up,
            decay_bias.reshape(1, -1),
            log_extra,
            head_gain.reshape(1, -1),
            mix_gain.reshape(1, -1),
            out_gain.reshape(1, -1),
            sums,
        )

    in_specs = (
        P(("grp", "fs"), "tp"),
        P("fs", "tp"),
        P("fs", "tp"),
        P("fs", "tp"),
        P(),
        P(),
        P(),
        P(("grp", "fs"), "tp"),
        P(),
        P("tp", "fs"),
        P("tp"),
        P("fs", "tp"),
        P("tp", "fs"),
        P("tp"),
    )
    out_specs = P(("grp", "fs"), "tp")
    return jax.shard_map(local, mesh=mesh, in_specs=in_specs, out_specs=out_specs, check_vma=False)
```

```python
import functools

import jax
import jax.numpy as jnp
import numpy as np
from jax import lax
from jax.experimental import pallas as pl
from jax.experimental.pallas import tpu as pltpu
from jax.sharding import PartitionSpec as P

DK = 128
DV = 256
TILE = 128
LEVELS = (64, 32, 16, 8, 4, 2, 1)
ALPHA = 2.0**0.5
TAU = 16.0
EPS = 1e-05
MESH = pl.DeviceIdType.MESH
BF = jnp.bfloat16
F32 = jnp.float32


def decay_sums():
    i = np.arange(TILE)[:, None]
    j = np.arange(TILE)[None, :]
    parts = []
    for m in LEVELS:
        mid = i // (2 * m) * (2 * m) + m - 1
        parts.append(np.where(i > mid, (j > mid) & (j <= i), (j > i) & (j <= mid)))
    parts.append(j <= i)
    parts.append(j > i)
    one = np.concatenate(parts, axis=0).astype(np.float32)
    return np.concatenate([one, one], axis=1)


def dot(a, b, dims=((1,), (0,))):
    return lax.dot_general(a, b, (dims, ((), ())), preferred_element_type=F32)


NT = ((1,), (1,))
TN = ((0,), (0,))
SIZES = (1.0, 0.5, 1.0, 1.0, 1.0, 1.0, 1.0, 1.0)
RANKS = (0, 1, 2, 3, 2, 2, 3, 3)
UNIT, DELAY, LEAD = 1.405, 2.0, 1.0
RECV, Z_SEND, Y_SEND = 0, 1, 2
ATTEND, MIXED, NORMED, UP_READY = 31.5, 40.0, 52.0, 64.0


def ring_plan(reach, shared):
    items, ready = [], []
    for d in range(2):
        waiting = [(0.0, p, 1) for p in range(len(reach))]
        free = 0.0
        while waiting:
            now = max(free, min(w[0] for w in waiting))
            best = min((w for w in waiting if w[0] <= now), key=lambda w: (RANKS[w[1]], w[0]))
            waiting.remove(best)
            since, p, h = best
            items.append((max(now - LEAD, since), Z_SEND, p, d, h))
            free = now + SIZES[p] * UNIT
            items.append((free + DELAY, RECV, p, d, h))
            if p < shared:
                ready.append((free + DELAY, p, d, h))
            if h < reach[p][d]:
                waiting.append((free + DELAY, p, h + 1))
    free = 0.0
    while ready:
        now = max(free, min(r[0] for r in ready))
        best = min((r for r in ready if r[0] <= now), key=lambda r: (r[1], r[0]))
        ready.remove(best)
        since, p, d, h = best
        items.append((max(now - LEAD, since), Y_SEND, p, d, h))
        free = now + SIZES[p] * UNIT
    return sorted(items)


def kernel(
    n_fs,
    n_tp,
    tokens,
    q_w,
    k_w,
    v_w,
    o_w,
    up_w,
    dn_w,
    fl,
    d_up,
    d_bias,
    extra,
    h_gain,
    m_gain,
    o_gain,
    sums,
    out,
    tok,
    wqkv,
    wo,
    wup,
    wdn,
    esum,
    mixed,
    part1,
    part2,
    pair_row,
    fwd_row_in,
    last_row_in,
    fwd_row_out,
    last_row_out,
    pair_col,
    fwd_col_in,
    last_col_in,
    fwd_col_out,
    last_col_out,
    nrm,
    act,
    stats,
    mg_all,
    local_sem,
    z_send,
    z_recv,
    y_send,
    y_recv,
    ag_send,
    ag_recv,
    rs_send,
    rs_recv,
    small_send,
    small_recv,
):
    z = lax.axis_index("fs")
    t = lax.axis_index("tp")
    grp = lax.axis_index("grp")
    g = lax.rem(grp, 2)
    mate = grp + 1 - 2 * g
    n_x = n_tp // 2
    x, c = t // 2, lax.rem(t, 2)
    right_t = 2 * lax.rem(x + 1, n_x) + c
    left_t = 2 * lax.rem(x + n_x - 1, n_x) + c
    across_t = 2 * lax.rem(x + 2, n_x) + c
    twin_t = t + 1 - 2 * c
    right_z = lax.rem(z + 1, n_fs)
    left_z = lax.rem(z + n_fs - 1, n_fs)
    rows = tok.shape[0]
    cols = tokens.shape[1]
    width = tok.shape[1]
    block = rows // n_tp
    zd = q_w.shape[0]

    def at(v, step):
        return pl.multiple_of(v * step, step)

    def remote(src, dst, ssem, rsem, dev):
        return pltpu.make_async_remote_copy(
            src_ref=src,
            dst_ref=dst,
            send_sem=ssem,
            recv_sem=rsem,
            device_id=dev,
            device_id_type=MESH,
        )

    pending = []

    def send(src, dst, ssem, rsem, dev):
        copy = remote(src, dst, ssem, rsem, dev)
        copy.start()
        pending.append(copy)

    def arrive(dst, ssem, rsem, dev):
        remote(dst, dst, ssem, rsem, dev).wait_recv()

    my_cols = pl.ds(at(z, zd), zd)
    kw = q_w.shape[1]
    vw = v_w.shape[1]
    own_rows = pl.ds(at(z, zd), zd)
    moves = [
        (q_w, wqkv.at[own_rows, pl.ds(0, kw)]),
        (k_w, wqkv.at[own_rows, pl.ds(kw, kw)]),
        (v_w, wqkv.at[own_rows, pl.ds(2 * kw, vw)]),
        (tokens, tok.at[:, pl.ds(at(t, cols), cols)]),
        (o_w, wo.at[:, my_cols]),
        (up_w, wup.at[own_rows, :]),
        (dn_w, wdn.at[:, my_cols]),
    ]
    moves = [pltpu.make_async_copy(s, d, local_sem.at[i]) for i, (s, d) in enumerate(moves)]
    for m in moves:
        m.start()

    barrier = pltpu.get_barrier_semaphore()
    peers = [{"fs": left_z}, {"fs": right_z}, {"grp": mate}]
    peers += [{"tp": lax.rem(t + k, n_tp)} for k in range(1, n_tp)]
    for p in peers:
        pl.semaphore_signal(barrier, inc=1, device_id=p, device_id_type=MESH)
    pl.semaphore_wait(barrier, len(peers))

    hq = zd // 2
    hu = zd // 4
    ho = wo.shape[0] // 2
    hd = wdn.shape[0] // 4

    def region(p, s, which):
        c0 = pl.ds(at(s, zd), zd)
        if p == 0:
            return wqkv.at[pl.ds(pl.multiple_of(s * zd + which * hq, hq), hq), :]
        if p == 1:
            return wo.at[pl.ds(at(which, ho), ho), c0]
        if p == 2:
            return wup.at[pl.ds(pl.multiple_of(s * zd + which * hu, hu), hu), :]
        if p == 3:
            return wdn.at[pl.ds(at(which, hd), hd), c0]
        if p in (4, 5):
            return wup.at[pl.ds(pl.multiple_of(s * zd + (p - 2) * hu, hu), hu), :]
        return wdn.at[pl.ds((p - 4) * hd, hd), c0]

    def whole(p):
        n = n_fs - 1
        if p == 0:
            return wqkv.at[pl.ds(0, n * hq), :]
        if p == 1:
            return wo.at[pl.ds(0, ho), pl.ds(0, n * zd)]
        if p in (2, 4, 5):
            return wup.at[pl.ds(0, n * hu), :]
        return wdn.at[pl.ds(0, hd), pl.ds(0, n * zd)]

    far = n_fs // 2
    near = n_fs - 1 - far
    reach = [(far, near) if p in (0, 2, 4, 6) else (near, far) for p in range(8)]

    def origin(d, h):
        return lax.rem(z + (n_fs - h if d == 0 else h), n_fs)

    def z_start(p, d, h):
        dev = {"fs": right_z if d == 0 else left_z}
        r = region(p, z if h == 1 else origin(d, h - 1), g)
        remote(r, r, z_send.at[p], z_recv.at[p, d, h - 1], dev).start()

    def z_event(p, d, h):
        dev = {"fs": left_z if d == 0 else right_z}
        arrive(region(p, origin(d, h), g), z_send.at[p], z_recv.at[p, d, h - 1], dev)

    def y_slot(d, h):
        return d * far + h - 1

    def y_start(p, d, h):
        r = region(p, origin(d, h), g)
        remote(r, r, y_send.at[p], y_recv.at[p, y_slot(d, h)], {"grp": mate}).start()

    def y_done(p):
        for d in range(2):
            for h in range(1, reach[p][d] + 1):
                r = region(p, origin(d, h), 1 - g)
                arrive(r, y_send.at[p], y_recv.at[p, y_slot(d, h)], {"grp": mate})

    steps = {RECV: z_event, Z_SEND: z_start, Y_SEND: y_start}
    order = ring_plan(reach, 4)
    done = [0]

    def pump(until):
        while done[0] < len(order) and order[done[0]][0] <= until:
            _, kind, p, d, h = order[done[0]]
            steps[kind](p, d, h)
            done[0] += 1

    def gather(i, view):
        ss, rs = ag_send.at[i], ag_recv.at[i]
        right, left, twin = {"tp": right_t}, {"tp": left_t}, {"tp": twin_t}

        def go(k, blk, half, dev):
            v = view(blk, half)
            send(v, v, ss.at[k], rs.at[k], dev)

        def got(k, blk, half, dev):
            arrive(view(blk, half), ss.at[k], rs.at[k], dev)

        flip = 1 - 2 * c

        def start():
            go(0, t, 0, right)
            go(2, t, 1, left)
            go(1, t, 1, right)
            go(3, t, 0, left)
            go(4, t, None, twin)

        def relay():
            got(0, left_t, 0, left)
            go(5, left_t, 0, right)
            got(2, right_t, 1, right)
            go(6, right_t, 1, left)

        def cross():
            got(1, left_t, 1, left)
            go(7, left_t, None, twin)
            got(3, right_t, 0, right)
            go(8, right_t, None, twin)

        def close():
            got(5, across_t, 0, left)
            go(9, across_t, 0, twin)
            got(6, across_t, 1, right)
            go(10, across_t, 1, twin)
            got(4, twin_t, None, twin)
            got(7, left_t + flip, None, twin)
            got(8, right_t + flip, None, twin)

        def finish():
            got(9, across_t + flip, 0, twin)
            got(10, across_t + flip, 1, twin)

        return start, relay, cross, close, finish

    def tok_view(blk, half):
        r = pl.ds(0, rows) if half is None else pl.ds(half * (rows // 2), rows // 2)
        return tok.at[r, pl.ds(at(blk, cols), cols)]

    def nrm_view(blk, half):
        cc = pl.ds(0, width) if half is None else pl.ds(half * (width // 2), width // 2)
        return nrm.at[pl.ds(at(blk, block), block), cc]

    rel = (2, 1, 0, 3)

    def scatter_sum(i, blk, bufs, cut, fill_twin, fill_own):
        ss, rs = rs_send.at[i], rs_recv.at[i]
        right, left, twin = {"tp": right_t}, {"tp": left_t}, {"tp": twin_t}
        pair_in, fwd_in, last_in, fwd_out, last_out = bufs
        for k in range(n_x):
            b = 2 * lax.rem(x + rel[k], n_x) + 1 - c
            fill_twin(b)
            send(blk(b), pair_in.at[k], ss.at[k], rs.at[k], twin)

        def pair(k):
            b = 2 * lax.rem(x + rel[k], n_x) + c
            fill_own(b)
            arrive(pair_in.at[k], ss.at[k], rs.at[k], twin)
            return blk(b)[...].astype(F32) + pair_in[k].astype(F32)

        def pass_on(src, dst, k, dev):
            send(src, dst, ss.at[k], rs.at[k], dev)

        s2 = pair(0)
        fwd_out[...] = s2.astype(BF)
        pass_on(cut(fwd_out, 0), fwd_in.at[0], 4, right)
        pass_on(cut(fwd_out, 1), fwd_in.at[1], 5, left)
        s1 = pair(1)
        last_out[0] = s1.astype(BF)
        pass_on(cut(last_out.at[0], 1), cut(last_in.at[0], 1), 6, right)
        s3 = pair(3)
        last_out[1] = s3.astype(BF)
        pass_on(cut(last_out.at[1], 0), cut(last_in.at[1], 0), 7, left)
        total = pair(2)
        yield
        arrive(fwd_in.at[0], ss.at[4], rs.at[4], left)
        head = cut(blk(2 * lax.rem(x + 1, n_x) + c), 0)[...].astype(F32)
        head = head + cut(pair_in.at[1], 0)[...].astype(F32) + fwd_in[0].astype(F32)
        cut(last_out.at[0], 0)[...] = head.astype(BF)
        pass_on(cut(last_out.at[0], 0), cut(last_in.at[0], 0), 8, right)
        arrive(fwd_in.at[1], ss.at[5], rs.at[5], right)
        head = cut(blk(2 * lax.rem(x + 3, n_x) + c), 1)[...].astype(F32)
        head = head + cut(pair_in.at[3], 1)[...].astype(F32) + fwd_in[1].astype(F32)
        cut(last_out.at[1], 1)[...] = head.astype(BF)
        pass_on(cut(last_out.at[1], 1), cut(last_in.at[1], 1), 9, left)
        yield
        for k, lo, dev in ((6, 0, left), (8, 0, left), (7, 1, right), (9, 1, right)):
            part = (1 if k == 6 else 0) if lo == 0 else (0 if k == 7 else 1)
            arrive(cut(last_in.at[lo], part), ss.at[k], rs.at[k], dev)
        yield total + last_in[0].astype(F32) + last_in[1].astype(F32)

    def row_block(b):
        return part1.at[pl.ds(at(b, block), block), :]

    def col_block(b):
        return part2.at[:, pl.ds(at(b, cols), cols)]

    def lane_half(ref, k):
        return ref.at[:, pl.ds(k * (width // 2), width // 2)]

    def row_half(ref, k):
        return ref.at[pl.ds(k * (rows // 2), rows // 2), :]

    def norm(v, gain):
        mean = jnp.mean(v, axis=1, keepdims=True)
        d = v - mean
        var = jnp.mean(d * d, axis=1, keepdims=True)
        return (d * lax.rsqrt(var + EPS) * gain).astype(BF)

    for i in (0, 1, 2, 3):
        moves[i].wait()
    tok_start, tok_relay, tok_cross, tok_close, tok_finish = gather(0, tok_view)
    pump(-0.5)
    for i in (4, 5, 6):
        moves[i].wait()
    pump(0.0)
    tok_start()
    mine = pl.ds(at(t, cols), cols)
    mg_all[:, mine] = m_gain[...]
    for k in range(1, n_tp):
        send(
            m_gain,
            mg_all.at[:, mine],
            small_send.at[0, k],
            small_recv.at[0, k],
            {"tp": lax.rem(t + k, n_tp)},
        )
    pump(5.5)
    tok_relay()
    pump(8.0)
    tok_cross()
    pump(10.8)
    tok_close()
    pump(12.0)
    tok_finish()

    key_cols = pl.ds(at(t, DK), DK)
    n_tiles = rows // TILE
    for i in range(n_tiles):
        rr = pl.ds(i * TILE, TILE)
        low = dot(tok[rr, :], fl[...], NT).astype(BF)
        pre = dot(low, d_up[:, key_cols]) + d_bias[:, key_cols]
        log_sig = jnp.minimum(pre, 0.0) - jnp.log1p(jnp.exp(-jnp.abs(pre)))
        decay = log_sig / TAU + extra[rr, :]
        hi = decay.astype(BF)
        lo = (decay - hi.astype(F32)).astype(BF)
        esum[i] = jnp.exp(dot(sums[...], jnp.concatenate([hi, lo], axis=0)))
        pump(13.0 + i)
    pump(ATTEND)
    y_done(0)

    ii = lax.broadcasted_iota(jnp.int32, (TILE, TILE), 0)
    jj = lax.broadcasted_iota(jnp.int32, (TILE, TILE), 1)
    state = jnp.zeros((DV, DK), F32)
    n_lv = len(LEVELS)
    for i in range(n_tiles):
        rr = pl.ds(i * TILE, TILE)
        qkv = dot(tok[rr, :], wqkv[...]).astype(BF)
        q = qkv[:, :DK].astype(F32) * DK**-0.5
        kb = qkv[:, DK : 2 * DK]
        k = kb.astype(F32)
        v = qkv[:, 2 * DK :]
        scores = jnp.where(ii == jj, dot(q.astype(BF), kb, NT), 0.0)
        for l, m in enumerate(LEVELS):
            e = esum[i, pl.ds(l * TILE, TILE), :]
            s = dot((q * e).astype(BF), (k * e).astype(BF), NT)
            scores = jnp.where(((ii ^ jj) // m == 1) & (ii > jj), s, scores)
        e_in = esum[i, pl.ds(n_lv * TILE, TILE), :]
        e_out = esum[i, pl.ds((n_lv + 1) * TILE, TILE), :]
        got = dot(scores.astype(BF), v)
        if i > 0:
            got = got + dot((q * e_in).astype(BF), state.astype(BF), NT)
        if i < n_tiles - 1:
            fresh = dot(v, (k * e_out).astype(BF), TN)
            state = state * e_in[TILE - 1 : TILE, :] + fresh
        scale = lax.rsqrt(jnp.mean(got * got, axis=1, keepdims=True) + EPS)
        mixed[rr, :] = (got * scale * h_gain[...]).astype(BF)
        pump(ATTEND + 1.3 * i + 1.0)
    pump(ATTEND + 5.5)
    y_done(1)

    step = 256

    def mix_cols(j, _):
        cc = pl.ds(pl.multiple_of(j * step, step), step)
        part1[:, cc] = dot(mixed[...], wo[:, cc]).astype(BF)
        return 0

    lax.fori_loop(0, width // step, mix_cols, 0)
    pump(MIXED)

    def nothing(b):
        pass

    row_bufs = (pair_row, fwd_row_in, last_row_in, fwd_row_out, last_row_out)
    rs1 = scatter_sum(0, row_block, row_bufs, lane_half, nothing, nothing)
    next(rs1)
    pump(MIXED + 5.5)
    next(rs1)
    for k in range(1, n_tp):
        src_t = lax.rem(t + n_tp - k, n_tp)
        arrive(
            mg_all.at[:, pl.ds(at(src_t, cols), cols)],
            small_send.at[0, k],
            small_recv.at[0, k],
            {"tp": src_t},
        )
    pump(MIXED + 9.5)
    mix = next(rs1)
    my_rows = pl.ds(at(t, block), block)
    nrm[my_rows, :] = norm(ALPHA * tok[my_rows, :].astype(F32) + mix, mg_all[...])
    n_start, n_relay, n_cross, n_close, n_finish = gather(1, nrm_view)
    n_start()
    pump(NORMED + 4.5)
    n_relay()
    pump(NORMED + 7.0)
    n_cross()
    pump(NORMED + 10.0)
    n_close()
    pump(NORMED + 11.0)
    n_finish()
    pump(UP_READY)
    y_done(2)
    n_up = act.shape[1] // step

    def up_cols(j, _):
        cc = pl.ds(pl.multiple_of(j * step, step), step)
        hidden = jnp.maximum(dot(nrm[...], wup[:, cc]), 0.0)
        act[:, cc] = (hidden * hidden).astype(BF)
        return 0

    lax.fori_loop(0, n_up // 2, up_cols, 0)
    pump(UP_READY + 2.0)
    lax.fori_loop(n_up // 2, n_up, up_cols, 0)
    pump(1e9)
    y_done(3)

    def down_block(b):
        cc = pl.ds(at(b, cols), cols)
        part2[:, cc] = dot(act[...], wdn[:, cc]).astype(BF)

    col_bufs = (pair_col, fwd_col_in, last_col_in, fwd_col_out, last_col_out)
    rs2 = scatter_sum(1, col_block, col_bufs, row_half, down_block, down_block)
    next(rs2)
    next(rs2)
    down = next(rs2)
    summed = ALPHA * nrm[:, mine].astype(F32) + down

    ones = jnp.ones((8, cols), BF)

    def row_sums(v):
        hi = v.astype(BF)
        lo = (v - hi.astype(F32)).astype(BF)
        return dot(ones, hi, NT) + dot(ones, lo, NT)

    odd = lax.broadcasted_iota(jnp.int32, (8, rows), 0) % 2 == 1
    stats[t] = jnp.where(odd, row_sums(summed * summed), row_sums(summed))
    for k in range(1, n_tp):
        send(
            stats.at[t],
            stats.at[t],
            small_send.at[1, k],
            small_recv.at[1, k],
            {"tp": lax.rem(t + k, n_tp)},
        )
    for k in range(1, n_tp):
        src_t = lax.rem(t + n_tp - k, n_tp)
        arrive(stats.at[src_t], small_send.at[1, k], small_recv.at[1, k], {"tp": src_t})
    both = stats[0]
    for k in range(1, n_tp):
        both = both + stats[k]
    both = jnp.transpose(both) / width
    mean, square = both[:, 0:1], both[:, 1:2]
    scale = lax.rsqrt(square - mean * mean + EPS)
    out[...] = ((summed - mean) * scale * o_gain[...]).astype(BF)
    for copy in pending:
        copy.wait_send()
    for p in range(8):
        w = whole(p)
        remote(w, w, z_send.at[p], z_recv.at[p, 0, 0], {"fs": right_z}).wait_send()
        if p < 4:
            remote(w, w, y_send.at[p], y_recv.at[p, 0], {"grp": mate}).wait_send()


def solution(mesh):
    n_fs, n_tp = mesh.shape["fs"], mesh.shape["tp"]
    assert n_tp == 8 and mesh.shape["grp"] % 2 == 0

    def local(
        tokens,
        query_matrix,
        key_weight,
        value_weight,
        forget_lower_factor,
        decay_up,
        decay_bias,
        log_extra,
        head_gain,
        out_weight,
        mix_gain,
        up_weight,
        down_weight,
        out_gain,
    ):
        rows, cols = tokens.shape
        width = cols * n_tp
        block = rows // n_tp
        zd = query_matrix.shape[0]
        hidden = up_weight.shape[1]
        vcols = value_weight.shape[1]
        qkv_cols = 2 * query_matrix.shape[1] + vcols
        sums = jnp.asarray(decay_sums(), BF)
        hbm = pl.BlockSpec(memory_space=pl.ANY)
        vmem = pl.BlockSpec(memory_space=pltpu.VMEM)
        far = n_fs // 2
        dma = pltpu.SemaphoreType.DMA
        return pl.pallas_call(
            functools.partial(kernel, n_fs, n_tp),
            out_shape=jax.ShapeDtypeStruct((rows, cols), BF),
            in_specs=[hbm] * 7 + [vmem] * 8,
            out_specs=vmem,
            scratch_shapes=[
                pltpu.VMEM((rows, width), BF),
                pltpu.VMEM((width, qkv_cols), BF),
                pltpu.VMEM((vcols, width), BF),
                pltpu.VMEM((width, hidden), BF),
                pltpu.VMEM((hidden, width), BF),
                pltpu.VMEM((rows // TILE, sums.shape[0], DK), F32),
                pltpu.VMEM((rows, vcols), BF),
                pltpu.VMEM((rows, width), BF),
                pltpu.VMEM((rows, width), BF),
                pltpu.VMEM((n_tp // 2, block, width), BF),
                pltpu.VMEM((2, block, width // 2), BF),
                pltpu.VMEM((2, block, width), BF),
                pltpu.VMEM((block, width), BF),
                pltpu.VMEM((2, block, width), BF),
                pltpu.VMEM((n_tp // 2, rows, cols), BF),
                pltpu.VMEM((2, rows // 2, cols), BF),
                pltpu.VMEM((2, rows, cols), BF),
                pltpu.VMEM((rows, cols), BF),
                pltpu.VMEM((2, rows, cols), BF),
                pltpu.VMEM((rows, width), BF),
                pltpu.VMEM((rows, hidden), BF),
                pltpu.VMEM((n_tp, 8, rows), F32),
                pltpu.VMEM((1, width), F32),
                dma((7,)),
                dma((8,)),
                dma((8, 2, far)),
                dma((4,)),
                dma((4, n_fs)),
                dma((2, 11)),
                dma((2, 11)),
                dma((2, 10)),
                dma((2, 10)),
                dma((2, n_tp)),
                dma((2, n_tp)),
            ],
            compiler_params=pltpu.CompilerParams(
                collective_id=0,
                has_side_effects=True,
                vmem_limit_bytes=60 * 1024 * 1024,
            ),
            name="layer",
        )(
            tokens,
            query_matrix,
            key_weight,
            value_weight,
            out_weight,
            up_weight,
            down_weight,
            forget_lower_factor.T,
            decay_up,
            decay_bias.reshape(1, -1),
            log_extra,
            head_gain.reshape(1, -1),
            mix_gain.reshape(1, -1),
            out_gain.reshape(1, -1),
            sums,
        )

    in_specs = (
        P(("grp", "fs"), "tp"),
        P("fs", "tp"),
        P("fs", "tp"),
        P("fs", "tp"),
        P(),
        P(),
        P(),
        P(("grp", "fs"), "tp"),
        P(),
        P("tp", "fs"),
        P("tp"),
        P("fs", "tp"),
        P("tp", "fs"),
        P("tp"),
    )
    out_specs = P(("grp", "fs"), "tp")
    return jax.shard_map(local, mesh=mesh, in_specs=in_specs, out_specs=out_specs, check_vma=False)
```

```python
import functools

import jax
import jax.numpy as jnp
import numpy as np
from jax import lax
from jax.experimental import pallas as pl
from jax.experimental.pallas import tpu as pltpu
from jax.sharding import PartitionSpec as P

DK = 128
DV = 256
TILE = 128
LEVELS = (64, 32, 16, 8, 4, 2, 1)
ALPHA = 2.0**0.5
TAU = 16.0
EPS = 1e-05
MESH = pl.DeviceIdType.MESH
BF = jnp.bfloat16
F32 = jnp.float32


def decay_sums():
    i = np.arange(TILE)[:, None]
    j = np.arange(TILE)[None, :]
    parts = []
    for m in LEVELS:
        mid = i // (2 * m) * (2 * m) + m - 1
        parts.append(np.where(i > mid, (j > mid) & (j <= i), (j > i) & (j <= mid)))
    parts.append(j <= i)
    parts.append(j > i)
    one = np.concatenate(parts, axis=0).astype(np.float32)
    return np.concatenate([one, one], axis=1)


def dot(a, b, dims=((1,), (0,))):
    return lax.dot_general(a, b, (dims, ((), ())), preferred_element_type=F32)


NT = ((1,), (1,))
TN = ((0,), (0,))
SIZES = (1.0, 0.5, 1.0, 1.0, 1.0, 1.0, 1.0, 1.0)
BIAS = (-100, -50, 0, 4, 0, 0, 4, 4)
UNIT, DELAY, LEAD = 1.405, 2.0, (1.0, 3.0)
RECV, Z_SEND, Y_SEND = 0, 1, 2
ATTEND, MIXED, NORMED, UP_READY, DOWN = 31.5, 41.0, 54.0, 70.0, 75.0


def ring_plan(reach, shared):
    items, ready = [], []
    for d in range(2):
        waiting = [(0.0, p, 1) for p in range(len(reach))]
        free = 0.0
        while waiting:
            now = max(free, min(w[0] for w in waiting))
            best = min((w for w in waiting if w[0] <= now), key=lambda w: (w[2] + BIAS[w[1]], w[0]))
            waiting.remove(best)
            since, p, h = best
            items.append((max(now - LEAD[now > 30], since), Z_SEND, p, d, h))
            free = now + SIZES[p] * UNIT
            items.append((free + DELAY, RECV, p, d, h))
            if p < shared:
                ready.append((free + DELAY, p, d, h))
            if h < reach[p][d]:
                waiting.append((free + DELAY, p, h + 1))
    free = 0.0
    while ready:
        now = max(free, min(r[0] for r in ready))
        best = min((r for r in ready if r[0] <= now), key=lambda r: (r[1], r[0]))
        ready.remove(best)
        since, p, d, h = best
        items.append((max(now - LEAD[now > 30], since), Y_SEND, p, d, h))
        free = now + SIZES[p] * UNIT
    return sorted(items)


def kernel(
    n_fs,
    n_tp,
    tokens,
    q_w,
    k_w,
    v_w,
    o_w,
    up_w,
    dn_w,
    fl_in,
    up_in,
    extra_in,
    sums_in,
    d_bias,
    h_gain,
    m_gain,
    o_gain,
    out,
    tok,
    wqkv,
    wo,
    wup,
    wdn,
    esum,
    mixed,
    part1,
    part2,
    pair_row,
    fwd_row_in,
    last_row_in,
    fwd_row_out,
    last_row_out,
    pair_col,
    fwd_col_in,
    last_col_in,
    fwd_col_out,
    last_col_out,
    nrm,
    act,
    stats,
    mg_all,
    fl,
    d_up,
    extra,
    sums,
    local_sem,
    z_send,
    z_recv,
    y_send,
    y_recv,
    ag_send,
    ag_recv,
    rs_send,
    rs_recv,
    small_send,
    small_recv,
):
    z = lax.axis_index("fs")
    t = lax.axis_index("tp")
    grp = lax.axis_index("grp")
    g = lax.rem(grp, 2)
    mate = grp + 1 - 2 * g
    n_x = n_tp // 2
    x, c = t // 2, lax.rem(t, 2)
    right_t = 2 * lax.rem(x + 1, n_x) + c
    left_t = 2 * lax.rem(x + n_x - 1, n_x) + c
    across_t = 2 * lax.rem(x + 2, n_x) + c
    twin_t = t + 1 - 2 * c
    right_z = lax.rem(z + 1, n_fs)
    left_z = lax.rem(z + n_fs - 1, n_fs)
    rows = tok.shape[0]
    cols = tokens.shape[1]
    width = tok.shape[1]
    block = rows // n_tp
    zd = q_w.shape[0]

    def at(v, step):
        return pl.multiple_of(v * step, step)

    def remote(src, dst, ssem, rsem, dev):
        return pltpu.make_async_remote_copy(
            src_ref=src,
            dst_ref=dst,
            send_sem=ssem,
            recv_sem=rsem,
            device_id=dev,
            device_id_type=MESH,
        )

    pending = []

    def send(src, dst, ssem, rsem, dev):
        copy = remote(src, dst, ssem, rsem, dev)
        copy.start()
        pending.append(copy)

    def arrive(dst, ssem, rsem, dev):
        remote(dst, dst, ssem, rsem, dev).wait_recv()

    barrier = pltpu.get_barrier_semaphore()
    peers = [{"fs": left_z}, {"fs": right_z}, {"grp": mate}]
    peers += [{"tp": lax.rem(t + k, n_tp)} for k in range(1, n_tp)]
    for p in peers:
        pl.semaphore_signal(barrier, inc=1, device_id=p, device_id_type=MESH)
    my_cols = pl.ds(at(z, zd), zd)
    kw = q_w.shape[1]
    vw = v_w.shape[1]
    own_rows = pl.ds(at(z, zd), zd)
    moves = [
        (q_w, wqkv.at[own_rows, pl.ds(0, kw)]),
        (k_w, wqkv.at[own_rows, pl.ds(kw, kw)]),
        (v_w, wqkv.at[own_rows, pl.ds(2 * kw, vw)]),
        (tokens, tok.at[:, pl.ds(at(t, cols), cols)]),
        (o_w, wo.at[:, my_cols]),
        (up_w, wup.at[own_rows, :]),
        (dn_w, wdn.at[:, my_cols]),
        (fl_in, fl),
        (up_in.at[:, pl.ds(at(t, DK), DK)], d_up),
        (extra_in, extra),
        (sums_in, sums),
    ]
    moves = [pltpu.make_async_copy(s, d, local_sem.at[i]) for i, (s, d) in enumerate(moves)]
    for m in moves:
        m.start()

    pl.semaphore_wait(barrier, len(peers))

    hq = zd // 2
    hu = zd // 4
    ho = wo.shape[0] // 2
    hd = wdn.shape[0] // 4

    def region(p, s, which):
        c0 = pl.ds(at(s, zd), zd)
        if p == 0:
            return wqkv.at[pl.ds(pl.multiple_of(s * zd + which * hq, hq), hq), :]
        if p == 1:
            return wo.at[pl.ds(at(which, ho), ho), c0]
        if p == 2:
            return wup.at[pl.ds(pl.multiple_of(s * zd + which * hu, hu), hu), :]
        if p == 3:
            return wdn.at[pl.ds(at(which, hd), hd), c0]
        if p in (4, 5):
            return wup.at[pl.ds(pl.multiple_of(s * zd + (p - 2) * hu, hu), hu), :]
        return wdn.at[pl.ds((p - 4) * hd, hd), c0]

    def whole(p):
        n = n_fs - 1
        if p == 0:
            return wqkv.at[pl.ds(0, n * hq), :]
        if p == 1:
            return wo.at[pl.ds(0, ho), pl.ds(0, n * zd)]
        if p in (2, 4, 5):
            return wup.at[pl.ds(0, n * hu), :]
        return wdn.at[pl.ds(0, hd), pl.ds(0, n * zd)]

    far = n_fs // 2
    near = n_fs - 1 - far
    reach = [(far, near) if p in (0, 2, 4, 6) else (near, far) for p in range(8)]

    def origin(d, h):
        return lax.rem(z + (n_fs - h if d == 0 else h), n_fs)

    def z_start(p, d, h):
        dev = {"fs": right_z if d == 0 else left_z}
        r = region(p, z if h == 1 else origin(d, h - 1), g)
        remote(r, r, z_send.at[p], z_recv.at[p, d, h - 1], dev).start()

    def z_event(p, d, h):
        dev = {"fs": left_z if d == 0 else right_z}
        arrive(region(p, origin(d, h), g), z_send.at[p], z_recv.at[p, d, h - 1], dev)

    def y_slot(d, h):
        return d * far + h - 1

    def y_start(p, d, h):
        r = region(p, origin(d, h), g)
        remote(r, r, y_send.at[p], y_recv.at[p, y_slot(d, h)], {"grp": mate}).start()

    def y_wait(p, d, h):
        r = region(p, origin(d, h), 1 - g)
        arrive(r, y_send.at[p], y_recv.at[p, y_slot(d, h)], {"grp": mate})

    def y_done(p):
        for d in range(2):
            for h in range(1, reach[p][d] + 1):
                y_wait(p, d, h)

    steps = {RECV: z_event, Z_SEND: z_start, Y_SEND: y_start}
    order = ring_plan(reach, 4)
    done = [0]

    def take():
        _, kind, p, d, h = order[done[0]]
        steps[kind](p, d, h)
        done[0] += 1

    def pump_hop(pieces, h):
        need = {(p, d) for p in pieces for d in range(2) if h <= reach[p][d]}
        while any(o[1] == RECV and o[4] == h and o[2:4] in need for o in order[done[0] :]):
            take()

    def pump(until):
        while done[0] < len(order) and order[done[0]][0] <= until:
            take()

    def gather(i, view):
        ss, rs = ag_send.at[i], ag_recv.at[i]
        right, left, twin = {"tp": right_t}, {"tp": left_t}, {"tp": twin_t}

        def go(k, blk, half, dev):
            v = view(blk, half)
            send(v, v, ss.at[k], rs.at[k], dev)

        def got(k, blk, half, dev):
            arrive(view(blk, half), ss.at[k], rs.at[k], dev)

        flip = 1 - 2 * c

        def start():
            go(0, t, 0, right)
            go(2, t, 1, left)
            go(1, t, 1, right)
            go(3, t, 0, left)
            go(4, t, None, twin)

        def relay():
            got(0, left_t, 0, left)
            go(5, left_t, 0, right)
            got(2, right_t, 1, right)
            go(6, right_t, 1, left)

        def cross():
            got(1, left_t, 1, left)
            go(7, left_t, None, twin)
            got(3, right_t, 0, right)
            go(8, right_t, None, twin)

        def close():
            got(5, across_t, 0, left)
            go(9, across_t, 0, twin)
            got(6, across_t, 1, right)
            go(10, across_t, 1, twin)
            got(4, twin_t, None, twin)
            got(7, left_t + flip, None, twin)
            got(8, right_t + flip, None, twin)

        def finish():
            got(9, across_t + flip, 0, twin)
            got(10, across_t + flip, 1, twin)

        return start, relay, cross, close, finish

    def tok_view(blk, half):
        r = pl.ds(0, rows) if half is None else pl.ds(half * (rows // 2), rows // 2)
        return tok.at[r, pl.ds(at(blk, cols), cols)]

    def nrm_view(blk, half):
        cc = pl.ds(0, width) if half is None else pl.ds(half * (width // 2), width // 2)
        return nrm.at[pl.ds(at(blk, block), block), cc]

    rel = (2, 1, 0, 3)

    def scatter_sum(i, blk, bufs, cut, fill_twin, fill_own):
        ss, rs = rs_send.at[i], rs_recv.at[i]
        right, left, twin = {"tp": right_t}, {"tp": left_t}, {"tp": twin_t}
        pair_in, fwd_in, last_in, fwd_out, last_out = bufs
        for k in range(n_x):
            b = 2 * lax.rem(x + rel[k], n_x) + 1 - c
            fill_twin(b)
            send(blk(b), pair_in.at[k], ss.at[k], rs.at[k], twin)

        def pair(k):
            b = 2 * lax.rem(x + rel[k], n_x) + c
            fill_own(b)
            arrive(pair_in.at[k], ss.at[k], rs.at[k], twin)
            return blk(b)[...].astype(F32) + pair_in[k].astype(F32)

        def pass_on(src, dst, k, dev):
            send(src, dst, ss.at[k], rs.at[k], dev)

        s2 = pair(0)
        fwd_out[...] = s2.astype(BF)
        pass_on(cut(fwd_out, 0), fwd_in.at[0], 4, right)
        pass_on(cut(fwd_out, 1), fwd_in.at[1], 5, left)
        s1 = pair(1)
        last_out[0] = s1.astype(BF)
        pass_on(cut(last_out.at[0], 1), cut(last_in.at[0], 1), 6, right)
        s3 = pair(3)
        last_out[1] = s3.astype(BF)
        pass_on(cut(last_out.at[1], 0), cut(last_in.at[1], 0), 7, left)
        total = pair(2)
        yield
        arrive(fwd_in.at[0], ss.at[4], rs.at[4], left)
        head = cut(blk(2 * lax.rem(x + 1, n_x) + c), 0)[...].astype(F32)
        head = head + cut(pair_in.at[1], 0)[...].astype(F32) + fwd_in[0].astype(F32)
        cut(last_out.at[0], 0)[...] = head.astype(BF)
        pass_on(cut(last_out.at[0], 0), cut(last_in.at[0], 0), 8, right)
        arrive(fwd_in.at[1], ss.at[5], rs.at[5], right)
        head = cut(blk(2 * lax.rem(x + 3, n_x) + c), 1)[...].astype(F32)
        head = head + cut(pair_in.at[3], 1)[...].astype(F32) + fwd_in[1].astype(F32)
        cut(last_out.at[1], 1)[...] = head.astype(BF)
        pass_on(cut(last_out.at[1], 1), cut(last_in.at[1], 1), 9, left)
        yield
        for k, lo, dev in ((6, 0, left), (8, 0, left), (7, 1, right), (9, 1, right)):
            part = (1 if k == 6 else 0) if lo == 0 else (0 if k == 7 else 1)
            arrive(cut(last_in.at[lo], part), ss.at[k], rs.at[k], dev)
        yield total + last_in[0].astype(F32) + last_in[1].astype(F32)

    def row_block(b):
        return part1.at[pl.ds(at(b, block), block), :]

    def col_block(b):
        return part2.at[:, pl.ds(at(b, cols), cols)]

    def lane_half(ref, k):
        return ref.at[:, pl.ds(k * (width // 2), width // 2)]

    def row_half(ref, k):
        return ref.at[pl.ds(k * (rows // 2), rows // 2), :]

    def norm(v, gain):
        mean = jnp.mean(v, axis=1, keepdims=True)
        d = v - mean
        var = jnp.mean(d * d, axis=1, keepdims=True)
        return (d * lax.rsqrt(var + EPS) * gain).astype(BF)

    for i in (0, 1, 2, 3):
        moves[i].wait()
    tok_start, tok_relay, tok_cross, tok_close, tok_finish = gather(0, tok_view)
    pump(-0.5)
    for i in (4, 5, 6):
        moves[i].wait()
    pump(0.0)
    tok_start()
    mine = pl.ds(at(t, cols), cols)
    mg_all[:, mine] = m_gain[...]
    for k in range(1, n_tp):
        send(
            m_gain,
            mg_all.at[:, mine],
            small_send.at[0, k],
            small_recv.at[0, k],
            {"tp": lax.rem(t + k, n_tp)},
        )
    pump(5.5)
    tok_relay()
    pump(8.0)
    tok_cross()
    pump(10.8)
    tok_close()
    pump(12.0)
    tok_finish()

    key_cols = pl.ds(at(t, DK), DK)
    n_tiles = rows // TILE
    for i in range(7, 11):
        moves[i].wait()
    for i in range(n_tiles):
        rr = pl.ds(i * TILE, TILE)
        low = dot(tok[rr, :], fl[...], NT).astype(BF)
        pre = dot(low, d_up[...]) + d_bias[:, key_cols]
        log_sig = jnp.minimum(pre, 0.0) - jnp.log1p(jnp.exp(-jnp.abs(pre)))
        decay = log_sig / TAU + extra[rr, :]
        hi = decay.astype(BF)
        lo = (decay - hi.astype(F32)).astype(BF)
        esum[i] = jnp.exp(dot(sums[...], jnp.concatenate([hi, lo], axis=0)))
        pump(13.0 + i)
    pump(ATTEND)
    y_done(0)

    ii = lax.broadcasted_iota(jnp.int32, (TILE, TILE), 0)
    jj = lax.broadcasted_iota(jnp.int32, (TILE, TILE), 1)
    state = jnp.zeros((DV, DK), F32)
    n_lv = len(LEVELS)
    for i in range(n_tiles):
        rr = pl.ds(i * TILE, TILE)
        qkv = dot(tok[rr, :], wqkv[...]).astype(BF)
        q = qkv[:, :DK].astype(F32) * DK**-0.5
        kb = qkv[:, DK : 2 * DK]
        k = kb.astype(F32)
        v = qkv[:, 2 * DK :]
        scores = jnp.where(ii == jj, dot(q.astype(BF), kb, NT), 0.0)
        for l, m in enumerate(LEVELS):
            e = esum[i, pl.ds(l * TILE, TILE), :]
            s = dot((q * e).astype(BF), (k * e).astype(BF), NT)
            scores = jnp.where(((ii ^ jj) // m == 1) & (ii > jj), s, scores)
        e_in = esum[i, pl.ds(n_lv * TILE, TILE), :]
        e_out = esum[i, pl.ds((n_lv + 1) * TILE, TILE), :]
        got = dot(scores.astype(BF), v)
        if i > 0:
            got = got + dot((q * e_in).astype(BF), state.astype(BF), NT)
        if i < n_tiles - 1:
            fresh = dot(v, (k * e_out).astype(BF), TN)
            state = state * e_in[TILE - 1 : TILE, :] + fresh
        scale = lax.rsqrt(jnp.mean(got * got, axis=1, keepdims=True) + EPS)
        mixed[rr, :] = (got * scale * h_gain[...]).astype(BF)
        pump(ATTEND + 1.3 * i + 1.0)
    pump(ATTEND + 5.5)
    y_done(1)

    step = 256

    def mix_cols(j, _):
        cc = pl.ds(pl.multiple_of(j * step, step), step)
        part1[:, cc] = dot(mixed[...], wo[:, cc]).astype(BF)
        return 0

    lax.fori_loop(0, width // step, mix_cols, 0)
    pump(MIXED)

    def nothing(b):
        pass

    row_bufs = (pair_row, fwd_row_in, last_row_in, fwd_row_out, last_row_out)
    rs1 = scatter_sum(0, row_block, row_bufs, lane_half, nothing, nothing)
    next(rs1)
    pump(MIXED + 5.5)
    next(rs1)
    for k in range(1, n_tp):
        src_t = lax.rem(t + n_tp - k, n_tp)
        arrive(
            mg_all.at[:, pl.ds(at(src_t, cols), cols)],
            small_send.at[0, k],
            small_recv.at[0, k],
            {"tp": src_t},
        )
    pump(MIXED + 9.5)
    mix = next(rs1)
    my_rows = pl.ds(at(t, block), block)
    nrm[my_rows, :] = norm(ALPHA * tok[my_rows, :].astype(F32) + mix, mg_all[...])
    n_start, n_relay, n_cross, n_close, n_finish = gather(1, nrm_view)
    n_start()
    pump(NORMED + 4.5)
    n_relay()
    pump(NORMED + 7.0)
    n_cross()
    pump(NORMED + 10.0)
    n_close()
    pump(NORMED + 11.0)
    n_finish()
    for copy in pending:
        copy.wait_send()
    pending.clear()
    pump(UP_READY)
    y_done(2)
    n_up = act.shape[1] // step

    def up_cols(j, _):
        cc = pl.ds(pl.multiple_of(j * step, step), step)
        hidden = jnp.maximum(dot(nrm[...], wup[:, cc]), 0.0)
        act[:, cc] = (hidden * hidden).astype(BF)
        return 0

    lax.fori_loop(0, n_up // 2, up_cols, 0)
    pump(UP_READY + 3.0)
    lax.fori_loop(n_up // 2, n_up, up_cols, 0)

    def down_origin(s):
        cc = pl.ds(at(s, zd), zd)
        part2[:, cc] = dot(act[...], wdn[:, cc]).astype(BF)

    down_origin(z)
    for h in range(1, far + 1):
        pump_hop((3, 6, 7), h)
        pump(DOWN + 1.4 * h)
        for d in range(2):
            if h <= reach[3][d]:
                y_wait(3, d, h)
        down_origin(origin(0, h))
        pump(DOWN + 1.4 * h + 0.7)
        if h <= near:
            down_origin(origin(1, h))
    pump(1e9)
    col_bufs = (pair_col, fwd_col_in, last_col_in, fwd_col_out, last_col_out)
    rs2 = scatter_sum(1, col_block, col_bufs, row_half, nothing, nothing)
    next(rs2)
    next(rs2)
    down = next(rs2)
    summed = ALPHA * nrm[:, mine].astype(F32) + down

    ones = jnp.ones((8, cols), BF)

    def row_sums(v):
        hi = v.astype(BF)
        lo = (v - hi.astype(F32)).astype(BF)
        return dot(ones, hi, NT) + dot(ones, lo, NT)

    stats[t, :, pl.ds(0, rows)] = row_sums(summed)[0:1, :]
    stats[t, :, pl.ds(rows, rows)] = row_sums(summed * summed)[0:1, :]
    for k in range(1, n_tp):
        send(
            stats.at[t],
            stats.at[t],
            small_send.at[1, k],
            small_recv.at[1, k],
            {"tp": lax.rem(t + k, n_tp)},
        )
    for k in range(1, n_tp):
        src_t = lax.rem(t + n_tp - k, n_tp)
        arrive(stats.at[src_t], small_send.at[1, k], small_recv.at[1, k], {"tp": src_t})
    both = stats[0]
    for k in range(1, n_tp):
        both = both + stats[k]
    first = lax.broadcasted_iota(jnp.int32, (8, rows), 0) == 0
    both = jnp.transpose(jnp.where(first, both[:, :rows], both[:, rows:])) / width
    mean, square = both[:, 0:1], both[:, 1:2]
    scale = lax.rsqrt(square - mean * mean + EPS)
    out[...] = ((summed - mean) * scale * o_gain[...]).astype(BF)
    for copy in pending:
        copy.wait_send()
    for p in range(8):
        w = whole(p)
        remote(w, w, z_send.at[p], z_recv.at[p, 0, 0], {"fs": right_z}).wait_send()
        if p < 4:
            remote(w, w, y_send.at[p], y_recv.at[p, 0], {"grp": mate}).wait_send()


def solution(mesh):
    n_fs, n_tp = mesh.shape["fs"], mesh.shape["tp"]
    assert n_tp == 8 and mesh.shape["grp"] % 2 == 0

    def local(
        tokens,
        query_matrix,
        key_weight,
        value_weight,
        forget_lower_factor,
        decay_up,
        decay_bias,
        log_extra,
        head_gain,
        out_weight,
        mix_gain,
        up_weight,
        down_weight,
        out_gain,
    ):
        rows, cols = tokens.shape
        width = cols * n_tp
        block = rows // n_tp
        zd = query_matrix.shape[0]
        hidden = up_weight.shape[1]
        vcols = value_weight.shape[1]
        qkv_cols = 2 * query_matrix.shape[1] + vcols
        sums = jnp.asarray(decay_sums(), BF)
        hbm = pl.BlockSpec(memory_space=pl.ANY)
        vmem = pl.BlockSpec(memory_space=pltpu.VMEM)
        far = n_fs // 2
        dma = pltpu.SemaphoreType.DMA
        return pl.pallas_call(
            functools.partial(kernel, n_fs, n_tp),
            out_shape=jax.ShapeDtypeStruct((rows, cols), BF),
            in_specs=[hbm] * 11 + [vmem] * 4,
            out_specs=vmem,
            scratch_shapes=[
                pltpu.VMEM((rows, width), BF),
                pltpu.VMEM((width, qkv_cols), BF),
                pltpu.VMEM((vcols, width), BF),
                pltpu.VMEM((width, hidden), BF),
                pltpu.VMEM((hidden, width), BF),
                pltpu.VMEM((rows // TILE, sums.shape[0], DK), F32),
                pltpu.VMEM((rows, vcols), BF),
                pltpu.VMEM((rows, width), BF),
                pltpu.VMEM((rows, width), BF),
                pltpu.VMEM((n_tp // 2, block, width), BF),
                pltpu.VMEM((2, block, width // 2), BF),
                pltpu.VMEM((2, block, width), BF),
                pltpu.VMEM((block, width), BF),
                pltpu.VMEM((2, block, width), BF),
                pltpu.VMEM((n_tp // 2, rows, cols), BF),
                pltpu.VMEM((2, rows // 2, cols), BF),
                pltpu.VMEM((2, rows, cols), BF),
                pltpu.VMEM((rows, cols), BF),
                pltpu.VMEM((2, rows, cols), BF),
                pltpu.VMEM((rows, width), BF),
                pltpu.VMEM((rows, hidden), BF),
                pltpu.VMEM((n_tp, 1, 2 * rows), F32),
                pltpu.VMEM((1, width), F32),
                pltpu.VMEM(forget_lower_factor.shape[::-1], BF),
                pltpu.VMEM((decay_up.shape[0], DK), BF),
                pltpu.VMEM(log_extra.shape, F32),
                pltpu.VMEM(sums.shape, BF),
                dma((11,)),
                dma((8,)),
                dma((8, 2, far)),
                dma((4,)),
                dma((4, n_fs)),
                dma((2, 11)),
                dma((2, 11)),
                dma((2, 10)),
                dma((2, 10)),
                dma((2, n_tp)),
                dma((2, n_tp)),
            ],
            compiler_params=pltpu.CompilerParams(
                collective_id=0,
                has_side_effects=True,
                vmem_limit_bytes=60 * 1024 * 1024,
            ),
            name="layer",
        )(
            tokens,
            query_matrix,
            key_weight,
            value_weight,
            out_weight,
            up_weight,
            down_weight,
            forget_lower_factor.T,
            decay_up,
            log_extra,
            sums,
            decay_bias.reshape(1, -1),
            head_gain.reshape(1, -1),
            mix_gain.reshape(1, -1),
            out_gain.reshape(1, -1),
        )

    in_specs = (
        P(("grp", "fs"), "tp"),
        P("fs", "tp"),
        P("fs", "tp"),
        P("fs", "tp"),
        P(),
        P(),
        P(),
        P(("grp", "fs"), "tp"),
        P(),
        P("tp", "fs"),
        P("tp"),
        P("fs", "tp"),
        P("tp", "fs"),
        P("tp"),
    )
    out_specs = P(("grp", "fs"), "tp")
    return jax.shard_map(local, mesh=mesh, in_specs=in_specs, out_specs=out_specs, check_vma=False)
```

```python
import functools

import jax
import jax.numpy as jnp
import numpy as np
from jax import lax
from jax.experimental import pallas as pl
from jax.experimental.pallas import tpu as pltpu
from jax.sharding import PartitionSpec as P

DK = 128
DV = 256
TILE = 128
LEVELS = (64, 32, 16, 8, 4, 2, 1)
ALPHA = 2.0**0.5
TAU = 16.0
EPS = 1e-05
MESH = pl.DeviceIdType.MESH
BF = jnp.bfloat16
F32 = jnp.float32


def decay_sums():
    i = np.arange(TILE)[:, None]
    j = np.arange(TILE)[None, :]
    parts = []
    for m in LEVELS:
        mid = i // (2 * m) * (2 * m) + m - 1
        parts.append(np.where(i > mid, (j > mid) & (j <= i), (j > i) & (j <= mid)))
    parts.append(j <= i)
    parts.append(j > i)
    one = np.concatenate(parts, axis=0).astype(np.float32)
    return np.concatenate([one, one], axis=1)


def dot(a, b, dims=((1,), (0,))):
    return lax.dot_general(a, b, (dims, ((), ())), preferred_element_type=F32)


NT = ((1,), (1,))
TN = ((0,), (0,))
SIZES = (1.0, 0.5, 1.0, 1.0, 1.0, 1.0, 1.0, 1.0)
BIAS = (-100, -50, 0, 4, 0, 0, 4, 4)
UNIT, DELAY, LEAD = 1.405, 2.0, (1.0, 3.0)
RECV, Z_SEND, Y_SEND = 0, 1, 2
ATTEND, MIXED, NORMED, UP_READY, DOWN = 31.5, 41.0, 54.0, 70.0, 75.0


def ring_plan(reach, shared):
    items, ready = [], []
    for d in range(2):
        waiting = [(0.0, p, 1) for p in range(len(reach))]
        free = 0.0
        while waiting:
            now = max(free, min(w[0] for w in waiting))
            best = min((w for w in waiting if w[0] <= now), key=lambda w: (w[2] + BIAS[w[1]], w[0]))
            waiting.remove(best)
            since, p, h = best
            items.append((max(now - LEAD[now > 30], since), Z_SEND, p, d, h))
            free = now + SIZES[p] * UNIT
            items.append((free + DELAY, RECV, p, d, h))
            if p < shared:
                ready.append((free + DELAY, p, d, h))
            if h < reach[p][d]:
                waiting.append((free + DELAY, p, h + 1))
    free = 0.0
    while ready:
        now = max(free, min(r[0] for r in ready))
        best = min((r for r in ready if r[0] <= now), key=lambda r: (r[1], r[0]))
        ready.remove(best)
        since, p, d, h = best
        items.append((max(now - LEAD[now > 30], since), Y_SEND, p, d, h))
        free = now + SIZES[p] * UNIT
    return sorted(items)


def kernel(
    n_fs,
    n_tp,
    tokens,
    q_w,
    k_w,
    v_w,
    o_w,
    up_w,
    dn_w,
    fl_in,
    up_in,
    extra_in,
    sums_in,
    d_bias,
    h_gain,
    m_gain,
    o_gain,
    out,
    tok,
    wqkv,
    wo,
    wup,
    wdn,
    esum,
    mixed,
    part1,
    part2,
    pair_row,
    fwd_row_in,
    last_row_in,
    fwd_row_out,
    last_row_out,
    pair_col,
    fwd_col_in,
    last_col_in,
    fwd_col_out,
    last_col_out,
    nrm,
    act,
    stats,
    mg_all,
    fl,
    d_up,
    extra,
    sums,
    local_sem,
    z_send,
    z_recv,
    y_send,
    y_recv,
    ag_send,
    ag_recv,
    rs_send,
    rs_recv,
    small_send,
    small_recv,
):
    z = lax.axis_index("fs")
    t = lax.axis_index("tp")
    grp = lax.axis_index("grp")
    g = lax.rem(grp, 2)
    mate = grp + 1 - 2 * g
    n_x = n_tp // 2
    x, c = t // 2, lax.rem(t, 2)
    right_t = 2 * lax.rem(x + 1, n_x) + c
    left_t = 2 * lax.rem(x + n_x - 1, n_x) + c
    across_t = 2 * lax.rem(x + 2, n_x) + c
    twin_t = t + 1 - 2 * c
    right_z = lax.rem(z + 1, n_fs)
    left_z = lax.rem(z + n_fs - 1, n_fs)
    rows = tok.shape[0]
    cols = tokens.shape[1]
    width = tok.shape[1]
    block = rows // n_tp
    zd = q_w.shape[0]

    def at(v, step):
        return pl.multiple_of(v * step, step)

    def remote(src, dst, ssem, rsem, dev):
        return pltpu.make_async_remote_copy(
            src_ref=src,
            dst_ref=dst,
            send_sem=ssem,
            recv_sem=rsem,
            device_id=dev,
            device_id_type=MESH,
        )

    def send(src, dst, ssem, rsem, dev):
        remote(src, dst, ssem, rsem, dev).start()

    def sent(amount, ssem, rsem):
        remote(amount, amount, ssem, rsem, {"tp": twin_t}).wait_send()

    def arrive(dst, ssem, rsem, dev):
        remote(dst, dst, ssem, rsem, dev).wait_recv()

    barrier = pltpu.get_barrier_semaphore()
    peers = [{"fs": left_z}, {"fs": right_z}, {"grp": mate}]
    peers += [{"tp": lax.rem(t + k, n_tp)} for k in range(1, n_tp)]
    for p in peers:
        pl.semaphore_signal(barrier, inc=1, device_id=p, device_id_type=MESH)
    my_cols = pl.ds(at(z, zd), zd)
    kw = q_w.shape[1]
    vw = v_w.shape[1]
    own_rows = pl.ds(at(z, zd), zd)
    moves = [
        (q_w, wqkv.at[own_rows, pl.ds(0, kw)]),
        (k_w, wqkv.at[own_rows, pl.ds(kw, kw)]),
        (v_w, wqkv.at[own_rows, pl.ds(2 * kw, vw)]),
        (tokens, tok.at[:, pl.ds(at(t, cols), cols)]),
        (o_w, wo.at[:, my_cols]),
        (up_w, wup.at[own_rows, :]),
        (dn_w, wdn.at[:, my_cols]),
        (fl_in, fl),
        (up_in.at[:, pl.ds(at(t, DK), DK)], d_up),
        (extra_in, extra),
        (sums_in, sums),
    ]
    moves = [pltpu.make_async_copy(s, d, local_sem.at[i]) for i, (s, d) in enumerate(moves)]
    for m in moves:
        m.start()

    pl.semaphore_wait(barrier, len(peers))

    hq = zd // 2
    hu = zd // 4
    ho = wo.shape[0] // 2
    hd = wdn.shape[0] // 4

    def region(p, s, which):
        c0 = pl.ds(at(s, zd), zd)
        if p == 0:
            return wqkv.at[pl.ds(pl.multiple_of(s * zd + which * hq, hq), hq), :]
        if p == 1:
            return wo.at[pl.ds(at(which, ho), ho), c0]
        if p == 2:
            return wup.at[pl.ds(pl.multiple_of(s * zd + which * hu, hu), hu), :]
        if p == 3:
            return wdn.at[pl.ds(at(which, hd), hd), c0]
        if p in (4, 5):
            return wup.at[pl.ds(pl.multiple_of(s * zd + (p - 2) * hu, hu), hu), :]
        return wdn.at[pl.ds((p - 4) * hd, hd), c0]

    def whole(p):
        n = n_fs - 1
        if p == 0:
            return wqkv.at[pl.ds(0, n * hq), :]
        if p == 1:
            return wo.at[pl.ds(0, ho), pl.ds(0, n * zd)]
        if p in (2, 4, 5):
            return wup.at[pl.ds(0, n * hu), :]
        return wdn.at[pl.ds(0, hd), pl.ds(0, n * zd)]

    far = n_fs // 2
    near = n_fs - 1 - far
    reach = [(far, near) if p in (0, 2, 4, 6) else (near, far) for p in range(8)]

    def origin(d, h):
        return lax.rem(z + (n_fs - h if d == 0 else h), n_fs)

    def z_start(p, d, h):
        dev = {"fs": right_z if d == 0 else left_z}
        r = region(p, z if h == 1 else origin(d, h - 1), g)
        remote(r, r, z_send.at[p], z_recv.at[p, d, h - 1], dev).start()

    def z_event(p, d, h):
        dev = {"fs": left_z if d == 0 else right_z}
        arrive(region(p, origin(d, h), g), z_send.at[p], z_recv.at[p, d, h - 1], dev)

    def y_slot(p, h):
        return p if p < 3 else 2 + h

    def y_start(p, d, h):
        r = region(p, origin(d, h), g)
        remote(r, r, y_send.at[p], y_recv.at[y_slot(p, h)], {"grp": mate}).start()

    def y_done(p):
        arrive(whole(p), y_send.at[p], y_recv.at[p], {"grp": mate})

    def y_wait(h):
        pair = wdn.at[pl.ds(0, hd), pl.ds(0, (2 if h <= near else 1) * zd)]
        arrive(pair, y_send.at[3], y_recv.at[2 + h], {"grp": mate})

    steps = {RECV: z_event, Z_SEND: z_start, Y_SEND: y_start}
    order = ring_plan(reach, 4)
    done = [0]

    def take():
        _, kind, p, d, h = order[done[0]]
        steps[kind](p, d, h)
        done[0] += 1

    def pump_hop(pieces, h):
        need = {(p, d) for p in pieces for d in range(2) if h <= reach[p][d]}
        while any(o[1] == RECV and o[4] == h and o[2:4] in need for o in order[done[0] :]):
            take()

    def pump(until):
        while done[0] < len(order) and order[done[0]][0] <= until:
            take()

    def gather(i, view):
        ss = ag_send.at[i]
        rs = ag_recv.at[i]
        right, left, twin = {"tp": right_t}, {"tp": left_t}, {"tp": twin_t}

        def go(k, blk, half, dev):
            v = view(blk, half)
            send(v, v, ss, rs.at[min(k, 6)], dev)

        def got(k, blk, half, dev):
            arrive(view(blk, half), ss, rs.at[k], dev)

        def start():
            go(0, t, 0, right)
            go(2, t, 1, left)
            go(1, t, 1, right)
            go(3, t, 0, left)
            go(6, t, None, twin)

        def relay():
            got(0, left_t, 0, left)
            go(4, left_t, 0, right)
            got(2, right_t, 1, right)
            go(5, right_t, 1, left)

        def cross():
            got(1, left_t, 1, left)
            go(7, left_t, None, twin)
            got(3, right_t, 0, right)
            go(8, right_t, None, twin)

        def close():
            got(4, across_t, 0, left)
            go(9, across_t, 0, twin)
            got(5, across_t, 1, right)
            go(10, across_t, 1, twin)

        def finish():
            arrive(tok.at[:, pl.ds(0, n_x * cols)], ss, rs.at[6], twin)

        return start, relay, cross, close, finish

    def tok_view(blk, half):
        r = pl.ds(0, rows) if half is None else pl.ds(half * (rows // 2), rows // 2)
        return tok.at[r, pl.ds(at(blk, cols), cols)]

    def nrm_view(blk, half):
        cc = pl.ds(0, width) if half is None else pl.ds(half * (width // 2), width // 2)
        return nrm.at[pl.ds(at(blk, block), block), cc]

    rel = (2, 1, 0, 3)

    def scatter_sum(i, blk, bufs, cut, fill_twin, fill_own):
        ss = rs_send.at[i]
        rs = rs_recv.at[i]
        right, left, twin = {"tp": right_t}, {"tp": left_t}, {"tp": twin_t}
        pair_in, fwd_in, last_in, fwd_out, last_out = bufs
        for k in range(n_x):
            b = 2 * lax.rem(x + rel[k], n_x) + 1 - c
            fill_twin(b)
            send(blk(b), pair_in.at[k], ss, rs.at[k], twin)

        def pair(k):
            b = 2 * lax.rem(x + rel[k], n_x) + c
            fill_own(b)
            arrive(pair_in.at[k], ss, rs.at[k], twin)
            return blk(b)[...].astype(F32) + pair_in[k].astype(F32)

        def pass_on(src, dst, k, dev):
            send(src, dst, ss, rs.at[min(k, 6)], dev)

        s2 = pair(0)
        fwd_out[...] = s2.astype(BF)
        pass_on(cut(fwd_out, 0), fwd_in.at[0], 4, right)
        pass_on(cut(fwd_out, 1), fwd_in.at[1], 5, left)
        s1 = pair(1)
        last_out[0] = s1.astype(BF)
        pass_on(cut(last_out.at[0], 1), cut(last_in.at[0], 1), 6, right)
        s3 = pair(3)
        last_out[1] = s3.astype(BF)
        pass_on(cut(last_out.at[1], 0), cut(last_in.at[1], 0), 7, left)
        total = pair(2)
        yield
        arrive(fwd_in.at[0], ss, rs.at[4], left)
        head = cut(blk(2 * lax.rem(x + 1, n_x) + c), 0)[...].astype(F32)
        head = head + cut(pair_in.at[1], 0)[...].astype(F32) + fwd_in[0].astype(F32)
        cut(last_out.at[0], 0)[...] = head.astype(BF)
        pass_on(cut(last_out.at[0], 0), cut(last_in.at[0], 0), 8, right)
        arrive(fwd_in.at[1], ss, rs.at[5], right)
        head = cut(blk(2 * lax.rem(x + 3, n_x) + c), 1)[...].astype(F32)
        head = head + cut(pair_in.at[3], 1)[...].astype(F32) + fwd_in[1].astype(F32)
        cut(last_out.at[1], 1)[...] = head.astype(BF)
        pass_on(cut(last_out.at[1], 1), cut(last_in.at[1], 1), 9, left)
        yield
        arrive(last_in, ss, rs.at[6], left)
        yield total + last_in[0].astype(F32) + last_in[1].astype(F32)

    def row_block(b):
        return part1.at[pl.ds(at(b, block), block), :]

    def col_block(b):
        return part2.at[:, pl.ds(at(b, cols), cols)]

    def lane_half(ref, k):
        return ref.at[:, pl.ds(k * (width // 2), width // 2)]

    def row_half(ref, k):
        return ref.at[pl.ds(k * (rows // 2), rows // 2), :]

    def norm(v, gain):
        mean = jnp.mean(v, axis=1, keepdims=True)
        d = v - mean
        var = jnp.mean(d * d, axis=1, keepdims=True)
        return (d * lax.rsqrt(var + EPS) * gain).astype(BF)

    for i in (0, 1, 2, 3):
        moves[i].wait()
    tok_start, tok_relay, tok_cross, tok_close, tok_finish = gather(0, tok_view)
    pump(-0.5)
    for i in (4, 5, 6):
        moves[i].wait()
    pump(0.0)
    tok_start()
    mine = pl.ds(at(t, cols), cols)
    mg_all[:, mine] = m_gain[...]
    for k in range(1, n_tp):
        send(
            m_gain,
            mg_all.at[:, mine],
            small_send.at[0],
            small_recv.at[0],
            {"tp": lax.rem(t + k, n_tp)},
        )
    pump(5.5)
    tok_relay()
    pump(8.0)
    tok_cross()
    pump(10.8)
    tok_close()
    pump(12.0)
    tok_finish()

    key_cols = pl.ds(at(t, DK), DK)
    n_tiles = rows // TILE
    for i in range(7, 11):
        moves[i].wait()
    for i in range(n_tiles):
        rr = pl.ds(i * TILE, TILE)
        low = dot(tok[rr, :], fl[...], NT).astype(BF)
        pre = dot(low, d_up[...]) + d_bias[:, key_cols]
        log_sig = jnp.minimum(pre, 0.0) - jnp.log1p(jnp.exp(-jnp.abs(pre)))
        decay = log_sig / TAU + extra[rr, :]
        hi = decay.astype(BF)
        lo = (decay - hi.astype(F32)).astype(BF)
        esum[i] = jnp.exp(dot(sums[...], jnp.concatenate([hi, lo], axis=0)))
        pump(13.0 + i)
    pump(ATTEND)
    y_done(0)

    ii = lax.broadcasted_iota(jnp.int32, (TILE, TILE), 0)
    jj = lax.broadcasted_iota(jnp.int32, (TILE, TILE), 1)
    state = jnp.zeros((DV, DK), F32)
    n_lv = len(LEVELS)
    for i in range(n_tiles):
        rr = pl.ds(i * TILE, TILE)
        qkv = dot(tok[rr, :], wqkv[...]).astype(BF)
        q = qkv[:, :DK].astype(F32) * DK**-0.5
        kb = qkv[:, DK : 2 * DK]
        k = kb.astype(F32)
        v = qkv[:, 2 * DK :]
        scores = jnp.where(ii == jj, dot(q.astype(BF), kb, NT), 0.0)
        for l, m in enumerate(LEVELS):
            e = esum[i, pl.ds(l * TILE, TILE), :]
            s = dot((q * e).astype(BF), (k * e).astype(BF), NT)
            scores = jnp.where(((ii ^ jj) // m == 1) & (ii > jj), s, scores)
        e_in = esum[i, pl.ds(n_lv * TILE, TILE), :]
        e_out = esum[i, pl.ds((n_lv + 1) * TILE, TILE), :]
        got = dot(scores.astype(BF), v)
        if i > 0:
            got = got + dot((q * e_in).astype(BF), state.astype(BF), NT)
        if i < n_tiles - 1:
            fresh = dot(v, (k * e_out).astype(BF), TN)
            state = state * e_in[TILE - 1 : TILE, :] + fresh
        scale = lax.rsqrt(jnp.mean(got * got, axis=1, keepdims=True) + EPS)
        mixed[rr, :] = (got * scale * h_gain[...]).astype(BF)
        pump(ATTEND + 1.3 * i + 1.0)
    pump(ATTEND + 5.5)
    y_done(1)

    step = 256

    def mix_cols(j, _):
        cc = pl.ds(pl.multiple_of(j * step, step), step)
        part1[:, cc] = dot(mixed[...], wo[:, cc]).astype(BF)
        return 0

    lax.fori_loop(0, width // step, mix_cols, 0)
    pump(MIXED)

    def nothing(b):
        pass

    row_bufs = (pair_row, fwd_row_in, last_row_in, fwd_row_out, last_row_out)
    rs1 = scatter_sum(0, row_block, row_bufs, lane_half, nothing, nothing)
    next(rs1)
    pump(MIXED + 5.5)
    next(rs1)
    gains = mg_all.at[:, pl.ds(0, (n_tp - 1) * cols)]
    arrive(gains, small_send.at[0], small_recv.at[0], {"tp": twin_t})
    pump(MIXED + 9.5)
    mix = next(rs1)
    my_rows = pl.ds(at(t, block), block)
    nrm[my_rows, :] = norm(ALPHA * tok[my_rows, :].astype(F32) + mix, mg_all[...])
    n_start, n_relay, n_cross, n_close, n_finish = gather(1, nrm_view)
    n_start()
    pump(NORMED + 4.5)
    n_relay()
    pump(NORMED + 7.0)
    n_cross()
    pump(NORMED + 10.0)
    n_close()
    pump(NORMED + 11.0)
    n_finish()
    most = pl.ds(0, (n_tp - 1) * cols)
    for i in range(2):
        sent(tok.at[:, most], ag_send.at[i], ag_recv.at[i, 0])
    sent(tok.at[:, most], rs_send.at[0], rs_recv.at[0, 0])
    sent(gains, small_send.at[0], small_recv.at[0])
    pump(UP_READY)
    y_done(2)
    n_up = act.shape[1] // step

    def up_cols(j, _):
        cc = pl.ds(pl.multiple_of(j * step, step), step)
        hidden = jnp.maximum(dot(nrm[...], wup[:, cc]), 0.0)
        act[:, cc] = (hidden * hidden).astype(BF)
        return 0

    lax.fori_loop(0, n_up // 2, up_cols, 0)
    pump(UP_READY + 3.0)
    lax.fori_loop(n_up // 2, n_up, up_cols, 0)

    def down_origin(s):
        cc = pl.ds(at(s, zd), zd)
        part2[:, cc] = dot(act[...], wdn[:, cc]).astype(BF)

    down_origin(z)
    for h in range(1, far + 1):
        pump_hop((3, 6, 7), h)
        pump(DOWN + 1.4 * h)
        y_wait(h)
        down_origin(origin(0, h))
        pump(DOWN + 1.4 * h + 0.7)
        if h <= near:
            down_origin(origin(1, h))
    pump(1e9)
    col_bufs = (pair_col, fwd_col_in, last_col_in, fwd_col_out, last_col_out)
    rs2 = scatter_sum(1, col_block, col_bufs, row_half, nothing, nothing)
    next(rs2)
    next(rs2)
    down = next(rs2)
    summed = ALPHA * nrm[:, mine].astype(F32) + down

    ones = jnp.ones((8, cols), BF)

    def row_sums(v):
        hi = v.astype(BF)
        lo = (v - hi.astype(F32)).astype(BF)
        return dot(ones, hi, NT) + dot(ones, lo, NT)

    stats[t, :, pl.ds(0, rows)] = row_sums(summed)[0:1, :]
    stats[t, :, pl.ds(rows, rows)] = row_sums(summed * summed)[0:1, :]
    for k in range(1, n_tp):
        send(
            stats.at[t],
            stats.at[t],
            small_send.at[1],
            small_recv.at[1],
            {"tp": lax.rem(t + k, n_tp)},
        )
    others = stats.at[pl.ds(0, n_tp - 1)]
    arrive(others, small_send.at[1], small_recv.at[1], {"tp": twin_t})
    both = stats[0]
    for k in range(1, n_tp):
        both = both + stats[k]
    first = lax.broadcasted_iota(jnp.int32, (8, rows), 0) == 0
    both = jnp.transpose(jnp.where(first, both[:, :rows], both[:, rows:])) / width
    mean, square = both[:, 0:1], both[:, 1:2]
    scale = lax.rsqrt(square - mean * mean + EPS)
    out[...] = ((summed - mean) * scale * o_gain[...]).astype(BF)
    sent(tok.at[:, most], rs_send.at[1], rs_recv.at[1, 0])
    sent(others, small_send.at[1], small_recv.at[1])
    for p in range(8):
        w = whole(p)
        remote(w, w, z_send.at[p], z_recv.at[p, 0, 0], {"fs": right_z}).wait_send()
        if p < 4:
            remote(w, w, y_send.at[p], y_recv.at[p], {"grp": mate}).wait_send()


def solution(mesh):
    n_fs, n_tp = mesh.shape["fs"], mesh.shape["tp"]
    assert n_tp == 8 and mesh.shape["grp"] % 2 == 0

    def local(
        tokens,
        query_matrix,
        key_weight,
        value_weight,
        forget_lower_factor,
        decay_up,
        decay_bias,
        log_extra,
        head_gain,
        out_weight,
        mix_gain,
        up_weight,
        down_weight,
        out_gain,
    ):
        rows, cols = tokens.shape
        width = cols * n_tp
        block = rows // n_tp
        zd = query_matrix.shape[0]
        hidden = up_weight.shape[1]
        vcols = value_weight.shape[1]
        qkv_cols = 2 * query_matrix.shape[1] + vcols
        sums = jnp.asarray(decay_sums(), BF)
        hbm = pl.BlockSpec(memory_space=pl.ANY)
        vmem = pl.BlockSpec(memory_space=pltpu.VMEM)
        far = n_fs // 2
        dma = pltpu.SemaphoreType.DMA
        return pl.pallas_call(
            functools.partial(kernel, n_fs, n_tp),
            out_shape=jax.ShapeDtypeStruct((rows, cols), BF),
            in_specs=[hbm] * 11 + [vmem] * 4,
            out_specs=vmem,
            scratch_shapes=[
                pltpu.VMEM((rows, width), BF),
                pltpu.VMEM((width, qkv_cols), BF),
                pltpu.VMEM((vcols, width), BF),
                pltpu.VMEM((width, hidden), BF),
                pltpu.VMEM((hidden, width), BF),
                pltpu.VMEM((rows // TILE, sums.shape[0], DK), F32),
                pltpu.VMEM((rows, vcols), BF),
                pltpu.VMEM((rows, width), BF),
                pltpu.VMEM((rows, width), BF),
                pltpu.VMEM((n_tp // 2, block, width), BF),
                pltpu.VMEM((2, block, width // 2), BF),
                pltpu.VMEM((2, block, width), BF),
                pltpu.VMEM((block, width), BF),
                pltpu.VMEM((2, block, width), BF),
                pltpu.VMEM((n_tp // 2, rows, cols), BF),
                pltpu.VMEM((2, rows // 2, cols), BF),
                pltpu.VMEM((2, rows, cols), BF),
                pltpu.VMEM((rows, cols), BF),
                pltpu.VMEM((2, rows, cols), BF),
                pltpu.VMEM((rows, width), BF),
                pltpu.VMEM((rows, hidden), BF),
                pltpu.VMEM((n_tp, 1, 2 * rows), F32),
                pltpu.VMEM((1, width), F32),
                pltpu.VMEM(forget_lower_factor.shape[::-1], BF),
                pltpu.VMEM((decay_up.shape[0], DK), BF),
                pltpu.VMEM(log_extra.shape, F32),
                pltpu.VMEM(sums.shape, BF),
                dma((11,)),
                dma((8,)),
                dma((8, 2, far)),
                dma((4,)),
                dma((3 + far,)),
                dma((2,)),
                dma((2, 7)),
                dma((2,)),
                dma((2, 7)),
                dma((2,)),
                dma((2,)),
            ],
            compiler_params=pltpu.CompilerParams(
                collective_id=0,
                has_side_effects=True,
                vmem_limit_bytes=60 * 1024 * 1024,
            ),
            name="layer",
        )(
            tokens,
            query_matrix,
            key_weight,
            value_weight,
            out_weight,
            up_weight,
            down_weight,
            forget_lower_factor.T,
            decay_up,
            log_extra,
            sums,
            decay_bias.reshape(1, -1),
            head_gain.reshape(1, -1),
            mix_gain.reshape(1, -1),
            out_gain.reshape(1, -1),
        )

    in_specs = (
        P(("grp", "fs"), "tp"),
        P("fs", "tp"),
        P("fs", "tp"),
        P("fs", "tp"),
        P(),
        P(),
        P(),
        P(("grp", "fs"), "tp"),
        P(),
        P("tp", "fs"),
        P("tp"),
        P("fs", "tp"),
        P("tp", "fs"),
        P("tp"),
    )
    out_specs = P(("grp", "fs"), "tp")
    return jax.shard_map(local, mesh=mesh, in_specs=in_specs, out_specs=out_specs, check_vma=False)
```

```python
import functools

import jax
import jax.numpy as jnp
import numpy as np
from jax import lax
from jax.experimental import pallas as pl
from jax.experimental.pallas import tpu as pltpu
from jax.sharding import PartitionSpec as P

DK = 128
DV = 256
TILE = 128
LEVELS = (64, 32, 16, 8, 4, 2, 1)
ALPHA = 2.0**0.5
TAU = 16.0
EPS = 1e-05
MESH = pl.DeviceIdType.MESH
BF = jnp.bfloat16
F32 = jnp.float32


def decay_sums():
    i = np.arange(TILE)[:, None]
    j = np.arange(TILE)[None, :]
    parts = []
    for m in LEVELS:
        mid = i // (2 * m) * (2 * m) + m - 1
        parts.append(np.where(i > mid, (j > mid) & (j <= i), (j > i) & (j <= mid)))
    parts.append(j <= i)
    parts.append(j > i)
    one = np.concatenate(parts, axis=0).astype(np.float32)
    return np.concatenate([one, one], axis=1)


def dot(a, b, dims=((1,), (0,))):
    return lax.dot_general(a, b, (dims, ((), ())), preferred_element_type=F32)


NT = ((1,), (1,))
TN = ((0,), (0,))
SIZES = (1.0, 0.5, 1.0, 1.0, 1.0, 1.0, 1.0, 1.0)
BIAS = (-100, -50, 0, 4, 0, 0, 4, 4)
UNIT, DELAY, LEAD = 1.405, 2.0, (1.0, 3.0)
RECV, Z_SEND, Y_SEND = 0, 1, 2
ATTEND, MIXED, NORMED, UP_READY, DOWN = 31.5, 41.0, 54.0, 70.0, 75.0


def ring_plan(reach, shared):
    items, ready = [], []
    for d in range(2):
        waiting = [(0.0, p, 1) for p in range(len(reach))]
        free = 0.0
        while waiting:
            now = max(free, min(w[0] for w in waiting))
            best = min((w for w in waiting if w[0] <= now), key=lambda w: (w[2] + BIAS[w[1]], w[0]))
            waiting.remove(best)
            since, p, h = best
            items.append((max(now - LEAD[now > 30], since), Z_SEND, p, d, h))
            free = now + SIZES[p] * UNIT
            items.append((free + DELAY, RECV, p, d, h))
            if p < shared:
                ready.append((free + DELAY, p, d, h))
            if h < reach[p][d]:
                waiting.append((free + DELAY, p, h + 1))
    free = 0.0
    while ready:
        now = max(free, min(r[0] for r in ready))
        best = min((r for r in ready if r[0] <= now), key=lambda r: (r[1], r[0]))
        ready.remove(best)
        since, p, d, h = best
        items.append((max(now - LEAD[now > 30], since), Y_SEND, p, d, h))
        free = now + SIZES[p] * UNIT
    return sorted(items)


def kernel(
    n_fs,
    n_tp,
    tokens,
    q_w,
    k_w,
    v_w,
    o_w,
    up_w,
    dn_w,
    fl_in,
    up_in,
    extra_in,
    sums_in,
    d_bias,
    h_gain,
    m_gain,
    o_gain,
    out,
    tok,
    wqkv,
    wo,
    wup,
    wdn,
    esum,
    mixed,
    part1,
    part2,
    pair_row,
    fwd_row_in,
    last_row_in,
    fwd_row_out,
    last_row_out,
    pair_col,
    fwd_col_in,
    last_col_in,
    fwd_col_out,
    last_col_out,
    nrm,
    act,
    stats,
    mg_all,
    fl,
    d_up,
    extra,
    sums,
    local_sem,
    z_send,
    z_recv,
    y_send,
    y_recv,
    ag_send,
    ag_recv,
    rs_send,
    rs_recv,
    small_send,
    small_recv,
):
    z = lax.axis_index("fs")
    t = lax.axis_index("tp")
    grp = lax.axis_index("grp")
    g = lax.rem(grp, 2)
    mate = grp + 1 - 2 * g
    n_x = n_tp // 2
    x, c = t // 2, lax.rem(t, 2)
    right_t = 2 * lax.rem(x + 1, n_x) + c
    left_t = 2 * lax.rem(x + n_x - 1, n_x) + c
    across_t = 2 * lax.rem(x + 2, n_x) + c
    twin_t = t + 1 - 2 * c
    right_z = lax.rem(z + 1, n_fs)
    left_z = lax.rem(z + n_fs - 1, n_fs)
    rows = tok.shape[0]
    cols = tokens.shape[1]
    width = tok.shape[1]
    block = rows // n_tp
    zd = q_w.shape[0]

    def at(v, step):
        return pl.multiple_of(v * step, step)

    def remote(src, dst, ssem, rsem, dev):
        return pltpu.make_async_remote_copy(
            src_ref=src,
            dst_ref=dst,
            send_sem=ssem,
            recv_sem=rsem,
            device_id=dev,
            device_id_type=MESH,
        )

    def send(src, dst, ssem, rsem, dev):
        remote(src, dst, ssem, rsem, dev).start()

    def sent(amount, ssem, rsem):
        remote(amount, amount, ssem, rsem, {"tp": twin_t}).wait_send()

    def arrive(dst, ssem, rsem, dev):
        remote(dst, dst, ssem, rsem, dev).wait_recv()

    barrier = pltpu.get_barrier_semaphore()
    peers = [{"fs": left_z}, {"fs": right_z}, {"grp": mate}]
    peers += [{"tp": lax.rem(t + k, n_tp)} for k in range(1, n_tp)]
    for p in peers:
        pl.semaphore_signal(barrier, inc=1, device_id=p, device_id_type=MESH)
    my_cols = pl.ds(at(z, zd), zd)
    kw = q_w.shape[1]
    vw = v_w.shape[1]
    own_rows = pl.ds(at(z, zd), zd)
    moves = [
        (q_w, wqkv.at[own_rows, pl.ds(0, kw)]),
        (k_w, wqkv.at[own_rows, pl.ds(kw, kw)]),
        (v_w, wqkv.at[own_rows, pl.ds(2 * kw, vw)]),
        (tokens, tok.at[:, pl.ds(at(t, cols), cols)]),
        (o_w, wo.at[:, my_cols]),
        (up_w, wup.at[own_rows, :]),
        (dn_w, wdn.at[:, my_cols]),
        (fl_in, fl),
        (up_in.at[:, pl.ds(at(t, DK), DK)], d_up),
        (extra_in, extra),
        (sums_in, sums),
    ]
    moves = [pltpu.make_async_copy(s, d, local_sem.at[i]) for i, (s, d) in enumerate(moves)]
    for m in moves:
        m.start()

    pl.semaphore_wait(barrier, len(peers))

    hq = zd // 2
    hu = zd // 4
    ho = wo.shape[0] // 2
    hd = wdn.shape[0] // 4

    def region(p, s, which):
        c0 = pl.ds(at(s, zd), zd)
        if p == 0:
            return wqkv.at[pl.ds(pl.multiple_of(s * zd + which * hq, hq), hq), :]
        if p == 1:
            return wo.at[pl.ds(at(which, ho), ho), c0]
        if p == 2:
            return wup.at[pl.ds(pl.multiple_of(s * zd + which * hu, hu), hu), :]
        if p == 3:
            return wdn.at[pl.ds(at(which, hd), hd), c0]
        if p in (4, 5):
            return wup.at[pl.ds(pl.multiple_of(s * zd + (p - 2) * hu, hu), hu), :]
        return wdn.at[pl.ds((p - 4) * hd, hd), c0]

    def whole(p):
        n = n_fs - 1
        if p == 0:
            return wqkv.at[pl.ds(0, n * hq), :]
        if p == 1:
            return wo.at[pl.ds(0, ho), pl.ds(0, n * zd)]
        if p in (2, 4, 5):
            return wup.at[pl.ds(0, n * hu), :]
        return wdn.at[pl.ds(0, hd), pl.ds(0, n * zd)]

    far = n_fs // 2
    near = n_fs - 1 - far
    reach = [(far, near) if p in (0, 2, 4, 6) else (near, far) for p in range(8)]

    def origin(d, h):
        return lax.rem(z + (n_fs - h if d == 0 else h), n_fs)

    def z_start(p, d, h):
        dev = {"fs": right_z if d == 0 else left_z}
        r = region(p, z if h == 1 else origin(d, h - 1), g)
        remote(r, r, z_send.at[p], z_recv.at[p, d, h - 1], dev).start()

    def z_event(p, d, h):
        dev = {"fs": left_z if d == 0 else right_z}
        arrive(region(p, origin(d, h), g), z_send.at[p], z_recv.at[p, d, h - 1], dev)

    def y_slot(p, h):
        return p if p < 3 else 2 + h

    def y_start(p, d, h):
        r = region(p, origin(d, h), g)
        remote(r, r, y_send.at[p], y_recv.at[y_slot(p, h)], {"grp": mate}).start()

    def y_done(p):
        arrive(whole(p), y_send.at[p], y_recv.at[p], {"grp": mate})

    def y_wait(h):
        pair = wdn.at[pl.ds(0, hd), pl.ds(0, (2 if h <= near else 1) * zd)]
        arrive(pair, y_send.at[3], y_recv.at[2 + h], {"grp": mate})

    steps = {RECV: z_event, Z_SEND: z_start, Y_SEND: y_start}
    order = ring_plan(reach, 4)
    done = [0]

    def take():
        _, kind, p, d, h = order[done[0]]
        steps[kind](p, d, h)
        done[0] += 1

    def pump_hop(pieces, h):
        need = {(p, d) for p in pieces for d in range(2) if h <= reach[p][d]}
        while any(o[1] == RECV and o[4] == h and o[2:4] in need for o in order[done[0] :]):
            take()

    def pump(until):
        while done[0] < len(order) and order[done[0]][0] <= until:
            take()

    def gather(i, view):
        ss = ag_send.at[i]
        rs = ag_recv.at[i]
        right, left, twin = {"tp": right_t}, {"tp": left_t}, {"tp": twin_t}

        def go(k, blk, half, dev):
            v = view(blk, half)
            send(v, v, ss, rs.at[min(k, 6)], dev)

        def got(k, blk, half, dev):
            arrive(view(blk, half), ss, rs.at[k], dev)

        def start():
            go(0, t, 0, right)
            go(2, t, 1, left)
            go(1, t, 1, right)
            go(3, t, 0, left)
            go(6, t, None, twin)

        def relay():
            got(0, left_t, 0, left)
            go(4, left_t, 0, right)
            got(2, right_t, 1, right)
            go(5, right_t, 1, left)

        def cross():
            got(1, left_t, 1, left)
            go(7, left_t, None, twin)
            got(3, right_t, 0, right)
            go(8, right_t, None, twin)

        def close():
            got(4, across_t, 0, left)
            go(9, across_t, 0, twin)
            got(5, across_t, 1, right)
            go(10, across_t, 1, twin)

        def finish():
            arrive(tok.at[:, pl.ds(0, n_x * cols)], ss, rs.at[6], twin)

        return start, relay, cross, close, finish

    def tok_view(blk, half):
        r = pl.ds(0, rows) if half is None else pl.ds(half * (rows // 2), rows // 2)
        return tok.at[r, pl.ds(at(blk, cols), cols)]

    def nrm_view(blk, half):
        cc = pl.ds(0, width) if half is None else pl.ds(half * (width // 2), width // 2)
        return nrm.at[pl.ds(at(blk, block), block), cc]

    rel = (2, 1, 0, 3)

    def scatter_sum(i, blk, bufs, cut, pair_at, collect):
        ss = rs_send.at[i]
        rs = rs_recv.at[i]
        right, left, twin = {"tp": right_t}, {"tp": left_t}, {"tp": twin_t}
        fwd_in, last_in, fwd_out, last_out = bufs

        def mine_at(k):
            return 2 * lax.rem(x + rel[k], n_x) + c

        def pair(k):
            collect(k)
            return blk(mine_at(k))[...].astype(F32) + pair_at(k)[...].astype(F32)

        def pass_on(src, dst, k, dev):
            send(src, dst, ss, rs.at[min(k, 6)], dev)

        s2 = pair(0)
        fwd_out[...] = s2.astype(BF)
        pass_on(cut(fwd_out, 0), fwd_in.at[0], 4, right)
        pass_on(cut(fwd_out, 1), fwd_in.at[1], 5, left)
        s1 = pair(1)
        last_out[0] = s1.astype(BF)
        pass_on(cut(last_out.at[0], 1), cut(last_in.at[0], 1), 6, right)
        s3 = pair(3)
        last_out[1] = s3.astype(BF)
        pass_on(cut(last_out.at[1], 0), cut(last_in.at[1], 0), 7, left)
        total = pair(2)
        yield
        arrive(fwd_in.at[0], ss, rs.at[4], left)
        head = cut(blk(mine_at(1)), 0)[...].astype(F32)
        head = head + cut(pair_at(1), 0)[...].astype(F32) + fwd_in[0].astype(F32)
        cut(last_out.at[0], 0)[...] = head.astype(BF)
        pass_on(cut(last_out.at[0], 0), cut(last_in.at[0], 0), 8, right)
        arrive(fwd_in.at[1], ss, rs.at[5], right)
        head = cut(blk(mine_at(3)), 1)[...].astype(F32)
        head = head + cut(pair_at(3), 1)[...].astype(F32) + fwd_in[1].astype(F32)
        cut(last_out.at[1], 1)[...] = head.astype(BF)
        pass_on(cut(last_out.at[1], 1), cut(last_in.at[1], 1), 9, left)
        yield
        arrive(last_in, ss, rs.at[6], left)
        yield total + last_in[0].astype(F32) + last_in[1].astype(F32)

    def row_block(b):
        return part1.at[pl.ds(at(b, block), block), :]

    def col_block(b):
        return part2.at[:, pl.ds(at(b, cols), cols)]

    def lane_half(ref, k):
        return ref.at[:, pl.ds(k * (width // 2), width // 2)]

    def row_half(ref, k):
        return ref.at[pl.ds(k * (rows // 2), rows // 2), :]

    def norm(v, gain):
        mean = jnp.mean(v, axis=1, keepdims=True)
        d = v - mean
        var = jnp.mean(d * d, axis=1, keepdims=True)
        return (d * lax.rsqrt(var + EPS) * gain).astype(BF)

    for i in (0, 1, 2, 3):
        moves[i].wait()
    tok_start, tok_relay, tok_cross, tok_close, tok_finish = gather(0, tok_view)
    pump(-0.5)
    for i in (4, 5, 6):
        moves[i].wait()
    pump(0.0)
    tok_start()
    mine = pl.ds(at(t, cols), cols)
    mg_all[:, mine] = m_gain[...]
    for k in range(1, n_tp):
        send(
            m_gain,
            mg_all.at[:, mine],
            small_send.at[0],
            small_recv.at[0],
            {"tp": lax.rem(t + k, n_tp)},
        )
    pump(5.5)
    tok_relay()
    pump(8.0)
    tok_cross()
    pump(10.8)
    tok_close()
    pump(12.0)
    tok_finish()

    key_cols = pl.ds(at(t, DK), DK)
    n_tiles = rows // TILE
    for i in range(7, 11):
        moves[i].wait()
    for i in range(n_tiles):
        rr = pl.ds(i * TILE, TILE)
        low = dot(tok[rr, :], fl[...], NT).astype(BF)
        pre = dot(low, d_up[...]) + d_bias[:, key_cols]
        log_sig = jnp.minimum(pre, 0.0) - jnp.log1p(jnp.exp(-jnp.abs(pre)))
        decay = log_sig / TAU + extra[rr, :]
        hi = decay.astype(BF)
        lo = (decay - hi.astype(F32)).astype(BF)
        esum[i] = jnp.exp(dot(sums[...], jnp.concatenate([hi, lo], axis=0)))
        pump(13.0 + i)
    pump(ATTEND)
    y_done(0)

    ii = lax.broadcasted_iota(jnp.int32, (TILE, TILE), 0)
    jj = lax.broadcasted_iota(jnp.int32, (TILE, TILE), 1)
    state = jnp.zeros((DV, DK), F32)
    n_lv = len(LEVELS)
    for i in range(n_tiles):
        rr = pl.ds(i * TILE, TILE)
        qkv = dot(tok[rr, :], wqkv[...]).astype(BF)
        q = qkv[:, :DK].astype(F32) * DK**-0.5
        kb = qkv[:, DK : 2 * DK]
        k = kb.astype(F32)
        v = qkv[:, 2 * DK :]
        scores = jnp.where(ii == jj, dot(q.astype(BF), kb, NT), 0.0)
        for l, m in enumerate(LEVELS):
            e = esum[i, pl.ds(l * TILE, TILE), :]
            s = dot((q * e).astype(BF), (k * e).astype(BF), NT)
            scores = jnp.where(((ii ^ jj) // m == 1) & (ii > jj), s, scores)
        e_in = esum[i, pl.ds(n_lv * TILE, TILE), :]
        e_out = esum[i, pl.ds((n_lv + 1) * TILE, TILE), :]
        got = dot(scores.astype(BF), v)
        if i > 0:
            got = got + dot((q * e_in).astype(BF), state.astype(BF), NT)
        if i < n_tiles - 1:
            fresh = dot(v, (k * e_out).astype(BF), TN)
            state = state * e_in[TILE - 1 : TILE, :] + fresh
        scale = lax.rsqrt(jnp.mean(got * got, axis=1, keepdims=True) + EPS)
        mixed[rr, :] = (got * scale * h_gain[...]).astype(BF)
        pump(ATTEND + 1.3 * i + 1.0)
    pump(ATTEND + 5.5)
    y_done(1)

    step = 256

    def mix_cols(j, _):
        cc = pl.ds(pl.multiple_of(j * step, step), step)
        part1[:, cc] = dot(mixed[...], wo[:, cc]).astype(BF)
        return 0

    lax.fori_loop(0, width // step, mix_cols, 0)
    pump(MIXED)

    for k in range(n_x):
        b = 2 * lax.rem(x + rel[k], n_x) + 1 - c
        send(row_block(b), pair_row.at[k], rs_send.at[0], rs_recv.at[0, k], {"tp": twin_t})

    def row_pair(k):
        return pair_row.at[k]

    def row_collect(k):
        arrive(pair_row.at[k], rs_send.at[0], rs_recv.at[0, k], {"tp": twin_t})

    row_bufs = (fwd_row_in, last_row_in, fwd_row_out, last_row_out)
    rs1 = scatter_sum(0, row_block, row_bufs, lane_half, row_pair, row_collect)
    next(rs1)
    pump(MIXED + 5.5)
    next(rs1)
    gains = mg_all.at[:, pl.ds(0, (n_tp - 1) * cols)]
    arrive(gains, small_send.at[0], small_recv.at[0], {"tp": twin_t})
    pump(MIXED + 9.5)
    mix = next(rs1)
    my_rows = pl.ds(at(t, block), block)
    nrm[my_rows, :] = norm(ALPHA * tok[my_rows, :].astype(F32) + mix, mg_all[...])
    n_start, n_relay, n_cross, n_close, n_finish = gather(1, nrm_view)
    n_start()
    pump(NORMED + 4.5)
    n_relay()
    pump(NORMED + 7.0)
    n_cross()
    pump(NORMED + 10.0)
    n_close()
    pump(NORMED + 11.0)
    n_finish()
    most = pl.ds(0, (n_tp - 1) * cols)
    for i in range(2):
        sent(tok.at[:, most], ag_send.at[i], ag_recv.at[i, 0])
    sent(tok.at[:, most], rs_send.at[0], rs_recv.at[0, 0])
    sent(gains, small_send.at[0], small_recv.at[0])
    pump(UP_READY)
    y_done(2)
    n_up = act.shape[1] // step

    def up_cols(j, _):
        cc = pl.ds(pl.multiple_of(j * step, step), step)
        hidden = jnp.maximum(dot(nrm[...], wup[:, cc]), 0.0)
        act[:, cc] = (hidden * hidden).astype(BF)
        return 0

    lax.fori_loop(0, n_up // 2, up_cols, 0)
    pump(UP_READY + 3.0)
    lax.fori_loop(n_up // 2, n_up, up_cols, 0)

    def down_origin(s):
        cc = pl.ds(at(s, zd), zd)
        part2[:, cc] = dot(act[...], wdn[:, cc]).astype(BF)

        @pl.when(lax.rem(s // (cols // zd), 2) != c)
        def _():
            send(part2.at[:, cc], pair_col.at[:, cc], rs_send.at[1], rs_recv.at[1, 0], {"tp": twin_t})

    down_origin(z)
    for h in range(1, far + 1):
        pump_hop((3, 6, 7), h)
        pump(DOWN + 1.4 * h)
        y_wait(h)
        down_origin(origin(0, h))
        pump(DOWN + 1.4 * h + 0.7)
        if h <= near:
            down_origin(origin(1, h))
    pump(1e9)

    def col_pair(k):
        return pair_col.at[:, pl.ds(at(2 * lax.rem(x + rel[k], n_x) + c, cols), cols)]

    def col_collect(k):
        if k == 0:
            half = pair_col.at[:, pl.ds(0, n_x * cols)]
            arrive(half, rs_send.at[1], rs_recv.at[1, 0], {"tp": twin_t})

    col_bufs = (fwd_col_in, last_col_in, fwd_col_out, last_col_out)
    rs2 = scatter_sum(1, col_block, col_bufs, row_half, col_pair, col_collect)
    next(rs2)
    next(rs2)
    down = next(rs2)
    summed = ALPHA * nrm[:, mine].astype(F32) + down

    ones = jnp.ones((8, cols), BF)

    def row_sums(v):
        hi = v.astype(BF)
        lo = (v - hi.astype(F32)).astype(BF)
        return dot(ones, hi, NT) + dot(ones, lo, NT)

    stats[t, :, pl.ds(0, rows)] = row_sums(summed)[0:1, :]
    stats[t, :, pl.ds(rows, rows)] = row_sums(summed * summed)[0:1, :]
    for k in range(1, n_tp):
        send(
            stats.at[t],
            stats.at[t],
            small_send.at[1],
            small_recv.at[1],
            {"tp": lax.rem(t + k, n_tp)},
        )
    others = stats.at[pl.ds(0, n_tp - 1)]
    arrive(others, small_send.at[1], small_recv.at[1], {"tp": twin_t})
    both = stats[0]
    for k in range(1, n_tp):
        both = both + stats[k]
    first = lax.broadcasted_iota(jnp.int32, (8, rows), 0) == 0
    both = jnp.transpose(jnp.where(first, both[:, :rows], both[:, rows:])) / width
    mean, square = both[:, 0:1], both[:, 1:2]
    scale = lax.rsqrt(square - mean * mean + EPS)
    out[...] = ((summed - mean) * scale * o_gain[...]).astype(BF)
    sent(tok.at[:, most], rs_send.at[1], rs_recv.at[1, 0])
    sent(others, small_send.at[1], small_recv.at[1])
    for p in range(8):
        w = whole(p)
        remote(w, w, z_send.at[p], z_recv.at[p, 0, 0], {"fs": right_z}).wait_send()
        if p < 4:
            remote(w, w, y_send.at[p], y_recv.at[p], {"grp": mate}).wait_send()


def solution(mesh):
    n_fs, n_tp = mesh.shape["fs"], mesh.shape["tp"]
    assert n_tp == 8 and mesh.shape["grp"] % 2 == 0

    def local(
        tokens,
        query_matrix,
        key_weight,
        value_weight,
        forget_lower_factor,
        decay_up,
        decay_bias,
        log_extra,
        head_gain,
        out_weight,
        mix_gain,
        up_weight,
        down_weight,
        out_gain,
    ):
        rows, cols = tokens.shape
        width = cols * n_tp
        block = rows // n_tp
        zd = query_matrix.shape[0]
        hidden = up_weight.shape[1]
        vcols = value_weight.shape[1]
        qkv_cols = 2 * query_matrix.shape[1] + vcols
        sums = jnp.asarray(decay_sums(), BF)
        hbm = pl.BlockSpec(memory_space=pl.ANY)
        vmem = pl.BlockSpec(memory_space=pltpu.VMEM)
        far = n_fs // 2
        dma = pltpu.SemaphoreType.DMA
        return pl.pallas_call(
            functools.partial(kernel, n_fs, n_tp),
            out_shape=jax.ShapeDtypeStruct((rows, cols), BF),
            in_specs=[hbm] * 11 + [vmem] * 4,
            out_specs=vmem,
            scratch_shapes=[
                pltpu.VMEM((rows, width), BF),
                pltpu.VMEM((width, qkv_cols), BF),
                pltpu.VMEM((vcols, width), BF),
                pltpu.VMEM((width, hidden), BF),
                pltpu.VMEM((hidden, width), BF),
                pltpu.VMEM((rows // TILE, sums.shape[0], DK), F32),
                pltpu.VMEM((rows, vcols), BF),
                pltpu.VMEM((rows, width), BF),
                pltpu.VMEM((rows, width), BF),
                pltpu.VMEM((n_tp // 2, block, width), BF),
                pltpu.VMEM((2, block, width // 2), BF),
                pltpu.VMEM((2, block, width), BF),
                pltpu.VMEM((block, width), BF),
                pltpu.VMEM((2, block, width), BF),
                pltpu.VMEM((rows, width), BF),
                pltpu.VMEM((2, rows // 2, cols), BF),
                pltpu.VMEM((2, rows, cols), BF),
                pltpu.VMEM((rows, cols), BF),
                pltpu.VMEM((2, rows, cols), BF),
                pltpu.VMEM((rows, width), BF),
                pltpu.VMEM((rows, hidden), BF),
                pltpu.VMEM((n_tp, 1, 2 * rows), F32),
                pltpu.VMEM((1, width), F32),
                pltpu.VMEM(forget_lower_factor.shape[::-1], BF),
                pltpu.VMEM((decay_up.shape[0], DK), BF),
                pltpu.VMEM(log_extra.shape, F32),
                pltpu.VMEM(sums.shape, BF),
                dma((11,)),
                dma((8,)),
                dma((8, 2, far)),
                dma((4,)),
                dma((3 + far,)),
                dma((2,)),
                dma((2, 7)),
                dma((2,)),
                dma((2, 7)),
                dma((2,)),
                dma((2,)),
            ],
            compiler_params=pltpu.CompilerParams(
                collective_id=0,
                has_side_effects=True,
                vmem_limit_bytes=60 * 1024 * 1024,
            ),
            name="layer",
        )(
            tokens,
            query_matrix,
            key_weight,
            value_weight,
            out_weight,
            up_weight,
            down_weight,
            forget_lower_factor.T,
            decay_up,
            log_extra,
            sums,
            decay_bias.reshape(1, -1),
            head_gain.reshape(1, -1),
            mix_gain.reshape(1, -1),
            out_gain.reshape(1, -1),
        )

    in_specs = (
        P(("grp", "fs"), "tp"),
        P("fs", "tp"),
        P("fs", "tp"),
        P("fs", "tp"),
        P(),
        P(),
        P(),
        P(("grp", "fs"), "tp"),
        P(),
        P("tp", "fs"),
        P("tp"),
        P("fs", "tp"),
        P("tp", "fs"),
        P("tp"),
    )
    out_specs = P(("grp", "fs"), "tp")
    return jax.shard_map(local, mesh=mesh, in_specs=in_specs, out_specs=out_specs, check_vma=False)
```

```python
import functools

import jax
import jax.numpy as jnp
import numpy as np
from jax import lax
from jax.experimental import pallas as pl
from jax.experimental.pallas import tpu as pltpu
from jax.sharding import PartitionSpec as P

DK = 128
DV = 256
TILE = 128
LEVELS = (64, 32, 16, 8, 4, 2, 1)
ALPHA = 2.0**0.5
TAU = 16.0
EPS = 1e-05
MESH = pl.DeviceIdType.MESH
BF = jnp.bfloat16
F32 = jnp.float32


def decay_sums():
    i = np.arange(TILE)[:, None]
    j = np.arange(TILE)[None, :]
    parts = []
    for m in LEVELS:
        mid = i // (2 * m) * (2 * m) + m - 1
        parts.append(np.where(i > mid, (j > mid) & (j <= i), (j > i) & (j <= mid)))
    parts.append(j <= i)
    parts.append(j > i)
    one = np.concatenate(parts, axis=0).astype(np.float32)
    return np.concatenate([one, one], axis=1)


def dot(a, b, dims=((1,), (0,))):
    return lax.dot_general(a, b, (dims, ((), ())), preferred_element_type=F32)


NT = ((1,), (1,))
TN = ((0,), (0,))
SIZES = (1.0, 0.5, 1.0, 1.0, 1.0, 1.0, 1.0, 1.0)
BIAS = (-100, -3, 0, 5, 0, 0, 5, 5)
UNIT, DELAY, LEAD = 1.405, 2.9, 2.0
RECV, Z_SEND, Y_SEND = 0, 1, 2
ATTEND, MIXED, NORMED, UP_READY, DOWN = 41.8, 50.2, 59.6, 70.0, 74.0


def ring_plan(reach, shared):
    items, ready = [], []
    for d in range(2):
        waiting = [(0.0, p, 1) for p in range(len(reach))]
        free = 0.0
        while waiting:
            now = max(free, min(w[0] for w in waiting))
            best = min((w for w in waiting if w[0] <= now), key=lambda w: (w[2] + BIAS[w[1]], w[0]))
            waiting.remove(best)
            since, p, h = best
            items.append((max(now - LEAD, since), Z_SEND, p, d, h))
            free = now + SIZES[p] * UNIT
            items.append((free + DELAY, RECV, p, d, h))
            if p < shared:
                ready.append((free + DELAY, p, d, h))
            if h < reach[p][d]:
                waiting.append((free + DELAY, p, h + 1))
    free = 0.0
    while ready:
        now = max(free, min(r[0] for r in ready))
        best = min((r for r in ready if r[0] <= now), key=lambda r: (r[1], r[0]))
        ready.remove(best)
        since, p, d, h = best
        items.append((max(now - LEAD, since), Y_SEND, p, d, h))
        free = now + SIZES[p] * UNIT
    return sorted(items)


def kernel(
    n_fs,
    n_tp,
    tokens,
    q_w,
    k_w,
    v_w,
    o_w,
    up_w,
    dn_w,
    fl_in,
    up_in,
    extra_in,
    sums_in,
    d_bias,
    h_gain,
    m_gain,
    o_gain,
    out,
    tok,
    wqkv,
    wo,
    wup,
    wdn,
    esum,
    mixed,
    part1,
    part2,
    pair_row,
    fwd_row_in,
    last_row_in,
    fwd_row_out,
    last_row_out,
    pair_col,
    fwd_col_in,
    last_col_in,
    fwd_col_out,
    last_col_out,
    nrm,
    act,
    stats,
    mg_all,
    fl,
    d_up,
    extra,
    sums,
    local_sem,
    z_send,
    z_recv,
    y_send,
    y_recv,
    ag_send,
    ag_recv,
    rs_send,
    rs_recv,
    small_send,
    small_recv,
):
    z = lax.axis_index("fs")
    t = lax.axis_index("tp")
    grp = lax.axis_index("grp")
    g = lax.rem(grp, 2)
    mate = grp + 1 - 2 * g
    n_x = n_tp // 2
    x, c = t // 2, lax.rem(t, 2)
    right_t = 2 * lax.rem(x + 1, n_x) + c
    left_t = 2 * lax.rem(x + n_x - 1, n_x) + c
    across_t = 2 * lax.rem(x + 2, n_x) + c
    twin_t = t + 1 - 2 * c
    right_z = lax.rem(z + 1, n_fs)
    left_z = lax.rem(z + n_fs - 1, n_fs)
    rows = tok.shape[0]
    cols = tokens.shape[1]
    width = tok.shape[1]
    block = rows // n_tp
    zd = q_w.shape[0]

    def at(v, step):
        return pl.multiple_of(v * step, step)

    def remote(src, dst, ssem, rsem, dev):
        return pltpu.make_async_remote_copy(
            src_ref=src,
            dst_ref=dst,
            send_sem=ssem,
            recv_sem=rsem,
            device_id=dev,
            device_id_type=MESH,
        )

    def send(src, dst, ssem, rsem, dev):
        remote(src, dst, ssem, rsem, dev).start()

    def sent(amount, ssem, rsem):
        remote(amount, amount, ssem, rsem, {"tp": twin_t}).wait_send()

    def arrive(dst, ssem, rsem, dev):
        remote(dst, dst, ssem, rsem, dev).wait_recv()

    barrier = pltpu.get_barrier_semaphore()
    peers = [{"fs": left_z}, {"fs": right_z}, {"grp": mate}]
    peers += [{"tp": lax.rem(t + k, n_tp)} for k in range(1, n_tp)]
    for p in peers:
        pl.semaphore_signal(barrier, inc=1, device_id=p, device_id_type=MESH)
    my_cols = pl.ds(at(z, zd), zd)
    kw = q_w.shape[1]
    vw = v_w.shape[1]
    own_rows = pl.ds(at(z, zd), zd)
    moves = [
        (q_w, wqkv.at[own_rows, pl.ds(0, kw)]),
        (k_w, wqkv.at[own_rows, pl.ds(kw, kw)]),
        (v_w, wqkv.at[own_rows, pl.ds(2 * kw, vw)]),
        (tokens, tok.at[:, pl.ds(at(t, cols), cols)]),
        (o_w, wo.at[:, my_cols]),
        (up_w, wup.at[own_rows, :]),
        (dn_w, wdn.at[:, my_cols]),
        (fl_in, fl),
        (up_in.at[:, pl.ds(at(t, DK), DK)], d_up),
        (extra_in, extra),
        (sums_in, sums),
    ]
    moves = [pltpu.make_async_copy(s, d, local_sem.at[i]) for i, (s, d) in enumerate(moves)]
    for m in moves:
        m.start()

    pl.semaphore_wait(barrier, len(peers))

    hq = zd // 2
    hu = zd // 4
    ho = wo.shape[0] // 2
    hd = wdn.shape[0] // 4

    def region(p, s, which):
        c0 = pl.ds(at(s, zd), zd)
        if p == 0:
            return wqkv.at[pl.ds(pl.multiple_of(s * zd + which * hq, hq), hq), :]
        if p == 1:
            return wo.at[pl.ds(at(which, ho), ho), c0]
        if p == 2:
            return wup.at[pl.ds(pl.multiple_of(s * zd + which * hu, hu), hu), :]
        if p == 3:
            return wdn.at[pl.ds(at(which, hd), hd), c0]
        if p in (4, 5):
            return wup.at[pl.ds(pl.multiple_of(s * zd + (p - 2) * hu, hu), hu), :]
        return wdn.at[pl.ds((p - 4) * hd, hd), c0]

    def whole(p):
        n = n_fs - 1
        if p == 0:
            return wqkv.at[pl.ds(0, n * hq), :]
        if p == 1:
            return wo.at[pl.ds(0, ho), pl.ds(0, n * zd)]
        if p in (2, 4, 5):
            return wup.at[pl.ds(0, n * hu), :]
        return wdn.at[pl.ds(0, hd), pl.ds(0, n * zd)]

    far = n_fs // 2
    near = n_fs - 1 - far
    reach = [(far, near) if p in (0, 2, 4, 6) else (near, far) for p in range(8)]

    def origin(d, h):
        return lax.rem(z + (n_fs - h if d == 0 else h), n_fs)

    def z_start(p, d, h):
        dev = {"fs": right_z if d == 0 else left_z}
        r = region(p, z if h == 1 else origin(d, h - 1), g)
        remote(r, r, z_send.at[p], z_recv.at[p, d, h - 1], dev).start()

    def z_event(p, d, h):
        dev = {"fs": left_z if d == 0 else right_z}
        arrive(region(p, origin(d, h), g), z_send.at[p], z_recv.at[p, d, h - 1], dev)

    def y_slot(p, h):
        return p if p < 3 else 2 + h

    def y_start(p, d, h):
        r = region(p, origin(d, h), g)
        remote(r, r, y_send.at[p], y_recv.at[y_slot(p, h)], {"grp": mate}).start()

    def y_done(p):
        arrive(whole(p), y_send.at[p], y_recv.at[p], {"grp": mate})

    def y_wait(h):
        pair = wdn.at[pl.ds(0, hd), pl.ds(0, (2 if h <= near else 1) * zd)]
        arrive(pair, y_send.at[3], y_recv.at[2 + h], {"grp": mate})

    steps = {RECV: z_event, Z_SEND: z_start, Y_SEND: y_start}
    order = ring_plan(reach, 4)
    done = [0]

    def take():
        _, kind, p, d, h = order[done[0]]
        steps[kind](p, d, h)
        done[0] += 1

    def pump_hop(pieces, h):
        need = {(p, d) for p in pieces for d in range(2) if h <= reach[p][d]}
        while any(o[1] == RECV and o[4] == h and o[2:4] in need for o in order[done[0] :]):
            take()

    def pump(until):
        while done[0] < len(order) and order[done[0]][0] <= until:
            take()

    def gather(i, view):
        ss = ag_send.at[i]
        rs = ag_recv.at[i]
        right, left, twin = {"tp": right_t}, {"tp": left_t}, {"tp": twin_t}

        def go(k, blk, half, dev):
            v = view(blk, half)
            send(v, v, ss, rs.at[min(k, 6)], dev)

        def got(k, blk, half, dev):
            arrive(view(blk, half), ss, rs.at[k], dev)

        def start():
            go(0, t, 0, right)
            go(2, t, 1, left)
            go(1, t, 1, right)
            go(3, t, 0, left)
            go(6, t, None, twin)

        def relay():
            got(0, left_t, 0, left)
            go(4, left_t, 0, right)
            got(2, right_t, 1, right)
            go(5, right_t, 1, left)

        def cross():
            got(1, left_t, 1, left)
            go(7, left_t, None, twin)
            got(3, right_t, 0, right)
            go(8, right_t, None, twin)

        def close():
            got(4, across_t, 0, left)
            go(9, across_t, 0, twin)
            got(5, across_t, 1, right)
            go(10, across_t, 1, twin)

        def finish():
            arrive(tok.at[:, pl.ds(0, n_x * cols)], ss, rs.at[6], twin)

        return start, relay, cross, close, finish

    def tok_view(blk, half):
        r = pl.ds(0, rows) if half is None else pl.ds(half * (rows // 2), rows // 2)
        return tok.at[r, pl.ds(at(blk, cols), cols)]

    def nrm_view(blk, half):
        cc = pl.ds(0, width) if half is None else pl.ds(half * (width // 2), width // 2)
        return nrm.at[pl.ds(at(blk, block), block), cc]

    rel = (2, 1, 0, 3)

    def scatter_sum(i, blk, bufs, cut, fill_twin, fill_own):
        ss = rs_send.at[i]
        rs = rs_recv.at[i]
        right, left, twin = {"tp": right_t}, {"tp": left_t}, {"tp": twin_t}
        pair_in, fwd_in, last_in, fwd_out, last_out = bufs
        for k in range(n_x):
            b = 2 * lax.rem(x + rel[k], n_x) + 1 - c
            fill_twin(b)
            send(blk(b), pair_in.at[k], ss, rs.at[k], twin)

        def pair(k):
            b = 2 * lax.rem(x + rel[k], n_x) + c
            fill_own(b)
            arrive(pair_in.at[k], ss, rs.at[k], twin)
            return blk(b)[...].astype(F32) + pair_in[k].astype(F32)

        def pass_on(src, dst, k, dev):
            send(src, dst, ss, rs.at[min(k, 6)], dev)

        s2 = pair(0)
        fwd_out[...] = s2.astype(BF)
        pass_on(cut(fwd_out, 0), fwd_in.at[0], 4, right)
        pass_on(cut(fwd_out, 1), fwd_in.at[1], 5, left)
        s1 = pair(1)
        last_out[0] = s1.astype(BF)
        pass_on(cut(last_out.at[0], 1), cut(last_in.at[0], 1), 6, right)
        s3 = pair(3)
        last_out[1] = s3.astype(BF)
        pass_on(cut(last_out.at[1], 0), cut(last_in.at[1], 0), 7, left)
        total = pair(2)
        yield
        arrive(fwd_in.at[0], ss, rs.at[4], left)
        head = cut(blk(2 * lax.rem(x + 1, n_x) + c), 0)[...].astype(F32)
        head = head + cut(pair_in.at[1], 0)[...].astype(F32) + fwd_in[0].astype(F32)
        cut(last_out.at[0], 0)[...] = head.astype(BF)
        pass_on(cut(last_out.at[0], 0), cut(last_in.at[0], 0), 8, right)
        arrive(fwd_in.at[1], ss, rs.at[5], right)
        head = cut(blk(2 * lax.rem(x + 3, n_x) + c), 1)[...].astype(F32)
        head = head + cut(pair_in.at[3], 1)[...].astype(F32) + fwd_in[1].astype(F32)
        cut(last_out.at[1], 1)[...] = head.astype(BF)
        pass_on(cut(last_out.at[1], 1), cut(last_in.at[1], 1), 9, left)
        yield
        arrive(last_in, ss, rs.at[6], left)
        yield total + last_in[0].astype(F32) + last_in[1].astype(F32)

    def row_block(b):
        return part1.at[pl.ds(at(b, block), block), :]

    def col_block(b):
        return part2.at[:, pl.ds(at(b, cols), cols)]

    def lane_half(ref, k):
        return ref.at[:, pl.ds(k * (width // 2), width // 2)]

    def row_half(ref, k):
        return ref.at[pl.ds(k * (rows // 2), rows // 2), :]

    def norm(v, gain):
        mean = jnp.mean(v, axis=1, keepdims=True)
        d = v - mean
        var = jnp.mean(d * d, axis=1, keepdims=True)
        return (d * lax.rsqrt(var + EPS) * gain).astype(BF)

    for i in (0, 1, 2, 3):
        moves[i].wait()
    tok_start, tok_relay, tok_cross, tok_close, tok_finish = gather(0, tok_view)
    pump(-0.5)
    for i in (4, 5, 6):
        moves[i].wait()
    pump(0.0)
    tok_start()
    mine = pl.ds(at(t, cols), cols)
    mg_all[:, mine] = m_gain[...]
    for k in range(1, n_tp):
        send(
            m_gain,
            mg_all.at[:, mine],
            small_send.at[0],
            small_recv.at[0],
            {"tp": lax.rem(t + k, n_tp)},
        )
    pump(5.5)
    tok_relay()
    pump(8.0)
    tok_cross()
    pump(10.8)
    tok_close()
    pump(12.0)
    tok_finish()

    key_cols = pl.ds(at(t, DK), DK)
    n_tiles = rows // TILE
    for i in range(7, 11):
        moves[i].wait()
    for i in range(n_tiles):
        rr = pl.ds(i * TILE, TILE)
        low = dot(tok[rr, :], fl[...], NT).astype(BF)
        pre = dot(low, d_up[...]) + d_bias[:, key_cols]
        log_sig = jnp.minimum(pre, 0.0) - jnp.log1p(jnp.exp(-jnp.abs(pre)))
        decay = log_sig / TAU + extra[rr, :]
        hi = decay.astype(BF)
        lo = (decay - hi.astype(F32)).astype(BF)
        esum[i] = jnp.exp(dot(sums[...], jnp.concatenate([hi, lo], axis=0)))
        pump(13.0 + i)
    pump(ATTEND)
    y_done(0)

    ii = lax.broadcasted_iota(jnp.int32, (TILE, TILE), 0)
    jj = lax.broadcasted_iota(jnp.int32, (TILE, TILE), 1)
    state = jnp.zeros((DV, DK), F32)
    n_lv = len(LEVELS)
    for i in range(n_tiles):
        rr = pl.ds(i * TILE, TILE)
        qkv = dot(tok[rr, :], wqkv[...]).astype(BF)
        q = qkv[:, :DK].astype(F32) * DK**-0.5
        kb = qkv[:, DK : 2 * DK]
        k = kb.astype(F32)
        v = qkv[:, 2 * DK :]
        scores = jnp.where(ii == jj, dot(q.astype(BF), kb, NT), 0.0)
        for l, m in enumerate(LEVELS):
            e = esum[i, pl.ds(l * TILE, TILE), :]
            s = dot((q * e).astype(BF), (k * e).astype(BF), NT)
            scores = jnp.where(((ii ^ jj) // m == 1) & (ii > jj), s, scores)
        e_in = esum[i, pl.ds(n_lv * TILE, TILE), :]
        e_out = esum[i, pl.ds((n_lv + 1) * TILE, TILE), :]
        got = dot(scores.astype(BF), v)
        if i > 0:
            got = got + dot((q * e_in).astype(BF), state.astype(BF), NT)
        if i < n_tiles - 1:
            fresh = dot(v, (k * e_out).astype(BF), TN)
            state = state * e_in[TILE - 1 : TILE, :] + fresh
        scale = lax.rsqrt(jnp.mean(got * got, axis=1, keepdims=True) + EPS)
        mixed[rr, :] = (got * scale * h_gain[...]).astype(BF)
        pump(ATTEND + 1.3 * i + 1.0)
    pump(ATTEND + 5.5)
    y_done(1)

    step = 256

    def mix_cols(j, _):
        cc = pl.ds(pl.multiple_of(j * step, step), step)
        part1[:, cc] = dot(mixed[...], wo[:, cc]).astype(BF)
        return 0

    lax.fori_loop(0, width // step, mix_cols, 0)
    pump(MIXED)

    def nothing(b):
        pass

    row_bufs = (pair_row, fwd_row_in, last_row_in, fwd_row_out, last_row_out)
    rs1 = scatter_sum(0, row_block, row_bufs, lane_half, nothing, nothing)
    next(rs1)
    pump(MIXED + 5.5)
    next(rs1)
    gains = mg_all.at[:, pl.ds(0, (n_tp - 1) * cols)]
    arrive(gains, small_send.at[0], small_recv.at[0], {"tp": twin_t})
    pump(MIXED + 9.5)
    mix = next(rs1)
    my_rows = pl.ds(at(t, block), block)
    nrm[my_rows, :] = norm(ALPHA * tok[my_rows, :].astype(F32) + mix, mg_all[...])
    n_start, n_relay, n_cross, n_close, n_finish = gather(1, nrm_view)
    n_start()
    pump(NORMED + 4.5)
    n_relay()
    pump(NORMED + 7.0)
    n_cross()
    pump(NORMED + 10.0)
    n_close()
    pump(NORMED + 11.0)
    n_finish()
    most = pl.ds(0, (n_tp - 1) * cols)
    for i in range(2):
        sent(tok.at[:, most], ag_send.at[i], ag_recv.at[i, 0])
    sent(tok.at[:, most], rs_send.at[0], rs_recv.at[0, 0])
    sent(gains, small_send.at[0], small_recv.at[0])
    pump(UP_READY)
    y_done(2)
    n_up = act.shape[1] // step

    def up_cols(j, _):
        cc = pl.ds(pl.multiple_of(j * step, step), step)
        hidden = jnp.maximum(dot(nrm[...], wup[:, cc]), 0.0)
        act[:, cc] = (hidden * hidden).astype(BF)
        return 0

    hops = [0]
    lax.fori_loop(0, n_up // 2, up_cols, 0)
    pump(UP_READY + 3.0)
    lax.fori_loop(n_up // 2, n_up, up_cols, 0)

    n_pairs = n_fs // 2
    for i, h in [(0, 1)] + [(k, min(2 * abs(k) + 1, far)) for m in range(1, far // 2) for k in (m, -m)] + [(far // 2, far)]:
        while hops[0] < h:
            hops[0] += 1
            pump_hop((3, 6, 7), hops[0])
            y_wait(hops[0])
        pump(DOWN + 1.2 * h)
        pair_at = lax.rem(z // 2 + i + n_pairs, n_pairs)
        cc = pl.ds(at(pair_at, 2 * zd), 2 * zd)
        part2[:, cc] = dot(act[...], wdn[:, cc]).astype(BF)
    pump(1e9)
    col_bufs = (pair_col, fwd_col_in, last_col_in, fwd_col_out, last_col_out)
    rs2 = scatter_sum(1, col_block, col_bufs, row_half, nothing, nothing)
    next(rs2)
    next(rs2)
    down = next(rs2)
    summed = ALPHA * nrm[:, mine].astype(F32) + down

    ones = jnp.ones((8, cols), BF)

    def row_sums(v):
        hi = v.astype(BF)
        lo = (v - hi.astype(F32)).astype(BF)
        return dot(ones, hi, NT) + dot(ones, lo, NT)

    stats[t, :, pl.ds(0, rows)] = row_sums(summed)[0:1, :]
    stats[t, :, pl.ds(rows, rows)] = row_sums(summed * summed)[0:1, :]
    for k in range(1, n_tp):
        send(
            stats.at[t],
            stats.at[t],
            small_send.at[1],
            small_recv.at[1],
            {"tp": lax.rem(t + k, n_tp)},
        )
    others = stats.at[pl.ds(0, n_tp - 1)]
    arrive(others, small_send.at[1], small_recv.at[1], {"tp": twin_t})
    both = stats[0]
    for k in range(1, n_tp):
        both = both + stats[k]
    first = lax.broadcasted_iota(jnp.int32, (8, rows), 0) == 0
    both = jnp.transpose(jnp.where(first, both[:, :rows], both[:, rows:])) / width
    mean, square = both[:, 0:1], both[:, 1:2]
    scale = lax.rsqrt(square - mean * mean + EPS)
    out[...] = ((summed - mean) * scale * o_gain[...]).astype(BF)
    sent(tok.at[:, most], rs_send.at[1], rs_recv.at[1, 0])
    sent(others, small_send.at[1], small_recv.at[1])
    for p in range(8):
        w = whole(p)
        remote(w, w, z_send.at[p], z_recv.at[p, 0, 0], {"fs": right_z}).wait_send()
        if p < 4:
            remote(w, w, y_send.at[p], y_recv.at[p], {"grp": mate}).wait_send()


def solution(mesh):
    n_fs, n_tp = mesh.shape["fs"], mesh.shape["tp"]
    assert n_tp == 8 and mesh.shape["grp"] % 2 == 0

    def local(
        tokens,
        query_matrix,
        key_weight,
        value_weight,
        forget_lower_factor,
        decay_up,
        decay_bias,
        log_extra,
        head_gain,
        out_weight,
        mix_gain,
        up_weight,
        down_weight,
        out_gain,
    ):
        rows, cols = tokens.shape
        width = cols * n_tp
        block = rows // n_tp
        zd = query_matrix.shape[0]
        hidden = up_weight.shape[1]
        vcols = value_weight.shape[1]
        qkv_cols = 2 * query_matrix.shape[1] + vcols
        sums = jnp.asarray(decay_sums(), BF)
        hbm = pl.BlockSpec(memory_space=pl.ANY)
        vmem = pl.BlockSpec(memory_space=pltpu.VMEM)
        far = n_fs // 2
        dma = pltpu.SemaphoreType.DMA
        return pl.pallas_call(
            functools.partial(kernel, n_fs, n_tp),
            out_shape=jax.ShapeDtypeStruct((rows, cols), BF),
            in_specs=[hbm] * 11 + [vmem] * 4,
            out_specs=vmem,
            scratch_shapes=[
                pltpu.VMEM((rows, width), BF),
                pltpu.VMEM((width, qkv_cols), BF),
                pltpu.VMEM((vcols, width), BF),
                pltpu.VMEM((width, hidden), BF),
                pltpu.VMEM((hidden, width), BF),
                pltpu.VMEM((rows // TILE, sums.shape[0], DK), F32),
                pltpu.VMEM((rows, vcols), BF),
                pltpu.VMEM((rows, width), BF),
                pltpu.VMEM((rows, width), BF),
                pltpu.VMEM((n_tp // 2, block, width), BF),
                pltpu.VMEM((2, block, width // 2), BF),
                pltpu.VMEM((2, block, width), BF),
                pltpu.VMEM((block, width), BF),
                pltpu.VMEM((2, block, width), BF),
                pltpu.VMEM((n_tp // 2, rows, cols), BF),
                pltpu.VMEM((2, rows // 2, cols), BF),
                pltpu.VMEM((2, rows, cols), BF),
                pltpu.VMEM((rows, cols), BF),
                pltpu.VMEM((2, rows, cols), BF),
                pltpu.VMEM((rows, width), BF),
                pltpu.VMEM((rows, hidden), BF),
                pltpu.VMEM((n_tp, 1, 2 * rows), F32),
                pltpu.VMEM((1, width), F32),
                pltpu.VMEM(forget_lower_factor.shape[::-1], BF),
                pltpu.VMEM((decay_up.shape[0], DK), BF),
                pltpu.VMEM(log_extra.shape, F32),
                pltpu.VMEM(sums.shape, BF),
                dma((11,)),
                dma((8,)),
                dma((8, 2, far)),
                dma((4,)),
                dma((3 + far,)),
                dma((2,)),
                dma((2, 7)),
                dma((2,)),
                dma((2, 7)),
                dma((2,)),
                dma((2,)),
            ],
            compiler_params=pltpu.CompilerParams(
                collective_id=0,
                has_side_effects=True,
                vmem_limit_bytes=60 * 1024 * 1024,
            ),
            name="layer",
        )(
            tokens,
            query_matrix,
            key_weight,
            value_weight,
            out_weight,
            up_weight,
            down_weight,
            forget_lower_factor.T,
            decay_up,
            log_extra,
            sums,
            decay_bias.reshape(1, -1),
            head_gain.reshape(1, -1),
            mix_gain.reshape(1, -1),
            out_gain.reshape(1, -1),
        )

    in_specs = (
        P(("grp", "fs"), "tp"),
        P("fs", "tp"),
        P("fs", "tp"),
        P("fs", "tp"),
        P(),
        P(),
        P(),
        P(("grp", "fs"), "tp"),
        P(),
        P("tp", "fs"),
        P("tp"),
        P("fs", "tp"),
        P("tp", "fs"),
        P("tp"),
    )
    out_specs = P(("grp", "fs"), "tp")
    return jax.shard_map(local, mesh=mesh, in_specs=in_specs, out_specs=out_specs, check_vma=False)
```

```python
import functools

import jax
import jax.numpy as jnp
import numpy as np
from jax import lax
from jax.experimental import pallas as pl
from jax.experimental.pallas import tpu as pltpu
from jax.sharding import PartitionSpec as P

DK = 128
DV = 256
TILE = 128
LEVELS = (64, 32, 16, 8, 4, 2, 1)
ALPHA = 2.0**0.5
TAU = 16.0
EPS = 1e-05
MESH = pl.DeviceIdType.MESH
BF = jnp.bfloat16
F32 = jnp.float32


def decay_sums():
    i = np.arange(TILE)[:, None]
    j = np.arange(TILE)[None, :]
    parts = []
    for m in LEVELS:
        mid = i // (2 * m) * (2 * m) + m - 1
        parts.append(np.where(i > mid, (j > mid) & (j <= i), (j > i) & (j <= mid)))
    parts.append(j <= i)
    parts.append(j > i)
    one = np.concatenate(parts, axis=0).astype(np.float32)
    return np.concatenate([one, one], axis=1)


def dot(a, b, dims=((1,), (0,))):
    return lax.dot_general(a, b, (dims, ((), ())), preferred_element_type=F32)


NT = ((1,), (1,))
TN = ((0,), (0,))
SIZES = (1.0, 0.5, 1.0, 1.0, 1.0, 1.0, 1.0, 1.0)
BIAS = (-100, -3, 0, 5, 0, 0, 5, 5)
UNIT, DELAY, LEAD = 1.405, 2.9, 2.0
RECV, Z_SEND, Y_SEND = 0, 1, 2
ATTEND, MIXED, NORMED, UP_READY, DOWN = 41.8, 51.0, 63.0, 76.0, 80.0


def ring_plan(reach, shared):
    items, ready = [], []
    for d in range(2):
        waiting = [(0.0, p, 1) for p in range(len(reach))]
        free = 0.0
        while waiting:
            now = max(free, min(w[0] for w in waiting))
            best = min((w for w in waiting if w[0] <= now), key=lambda w: (w[2] + BIAS[w[1]], w[0]))
            waiting.remove(best)
            since, p, h = best
            items.append((max(now - LEAD, since), Z_SEND, p, d, h))
            free = now + SIZES[p] * UNIT
            items.append((free + DELAY, RECV, p, d, h))
            if p < shared:
                ready.append((free + DELAY, p, d, h))
            if h < reach[p][d]:
                waiting.append((free + DELAY, p, h + 1))
    free = 0.0
    while ready:
        now = max(free, min(r[0] for r in ready))
        best = min((r for r in ready if r[0] <= now), key=lambda r: (r[1], r[0]))
        ready.remove(best)
        since, p, d, h = best
        items.append((max(now - LEAD, since), Y_SEND, p, d, h))
        free = now + SIZES[p] * UNIT
    return sorted(items)


def kernel(
    n_fs,
    n_tp,
    tokens,
    q_w,
    k_w,
    v_w,
    o_w,
    up_w,
    dn_w,
    fl_in,
    up_in,
    extra_in,
    sums_in,
    d_bias,
    h_gain,
    m_gain,
    o_gain,
    out,
    tok,
    wqkv,
    wo,
    wup,
    wdn,
    esum,
    mixed,
    part1,
    part2,
    pair_row,
    fwd_row_in,
    last_row_in,
    fwd_row_out,
    last_row_out,
    pair_col,
    fwd_col_in,
    last_col_in,
    fwd_col_out,
    last_col_out,
    nrm,
    act,
    stats,
    mg_all,
    fl,
    d_up,
    extra,
    sums,
    local_sem,
    z_send,
    z_recv,
    y_send,
    y_recv,
    ag_send,
    ag_recv,
    rs_send,
    rs_recv,
    small_send,
    small_recv,
):
    z = lax.axis_index("fs")
    t = lax.axis_index("tp")
    grp = lax.axis_index("grp")
    g = lax.rem(grp, 2)
    mate = grp + 1 - 2 * g
    n_x = n_tp // 2
    x, c = t // 2, lax.rem(t, 2)
    right_t = 2 * lax.rem(x + 1, n_x) + c
    left_t = 2 * lax.rem(x + n_x - 1, n_x) + c
    across_t = 2 * lax.rem(x + 2, n_x) + c
    twin_t = t + 1 - 2 * c
    right_z = lax.rem(z + 1, n_fs)
    left_z = lax.rem(z + n_fs - 1, n_fs)
    rows = tok.shape[0]
    cols = tokens.shape[1]
    width = tok.shape[1]
    block = rows // n_tp
    zd = q_w.shape[0]

    def at(v, step):
        return pl.multiple_of(v * step, step)

    def remote(src, dst, ssem, rsem, dev):
        return pltpu.make_async_remote_copy(
            src_ref=src,
            dst_ref=dst,
            send_sem=ssem,
            recv_sem=rsem,
            device_id=dev,
            device_id_type=MESH,
        )

    def send(src, dst, ssem, rsem, dev):
        remote(src, dst, ssem, rsem, dev).start()

    def sent(amount, ssem, rsem):
        remote(amount, amount, ssem, rsem, {"tp": twin_t}).wait_send()

    def arrive(dst, ssem, rsem, dev):
        remote(dst, dst, ssem, rsem, dev).wait_recv()

    barrier = pltpu.get_barrier_semaphore()
    peers = [{"fs": left_z}, {"fs": right_z}, {"grp": mate}]
    peers += [{"tp": lax.rem(t + k, n_tp)} for k in range(1, n_tp)]
    for p in peers:
        pl.semaphore_signal(barrier, inc=1, device_id=p, device_id_type=MESH)
    my_cols = pl.ds(at(z, zd), zd)
    kw = q_w.shape[1]
    vw = v_w.shape[1]
    own_rows = pl.ds(at(z, zd), zd)
    moves = [
        (q_w, wqkv.at[own_rows, pl.ds(0, kw)]),
        (k_w, wqkv.at[own_rows, pl.ds(kw, kw)]),
        (v_w, wqkv.at[own_rows, pl.ds(2 * kw, vw)]),
        (tokens, tok.at[:, pl.ds(at(t, cols), cols)]),
        (o_w, wo.at[:, my_cols]),
        (up_w, wup.at[own_rows, :]),
        (dn_w, wdn.at[:, my_cols]),
        (fl_in, fl),
        (up_in.at[:, pl.ds(at(t, DK), DK)], d_up),
        (extra_in, extra),
        (sums_in, sums),
    ]
    moves = [pltpu.make_async_copy(s, d, local_sem.at[i]) for i, (s, d) in enumerate(moves)]
    for m in moves:
        m.start()

    pl.semaphore_wait(barrier, len(peers))

    hq = zd // 2
    hu = zd // 4
    ho = wo.shape[0] // 2
    hd = wdn.shape[0] // 4

    def region(p, s, which):
        c0 = pl.ds(at(s, zd), zd)
        if p == 0:
            return wqkv.at[pl.ds(pl.multiple_of(s * zd + which * hq, hq), hq), :]
        if p == 1:
            return wo.at[pl.ds(at(which, ho), ho), c0]
        if p == 2:
            return wup.at[pl.ds(pl.multiple_of(s * zd + which * hu, hu), hu), :]
        if p == 3:
            return wdn.at[pl.ds(at(which, hd), hd), c0]
        if p in (4, 5):
            return wup.at[pl.ds(pl.multiple_of(s * zd + (p - 2) * hu, hu), hu), :]
        return wdn.at[pl.ds((p - 4) * hd, hd), c0]

    def whole(p):
        n = n_fs - 1
        if p == 0:
            return wqkv.at[pl.ds(0, n * hq), :]
        if p == 1:
            return wo.at[pl.ds(0, ho), pl.ds(0, n * zd)]
        if p in (2, 4, 5):
            return wup.at[pl.ds(0, n * hu), :]
        return wdn.at[pl.ds(0, hd), pl.ds(0, n * zd)]

    far = n_fs // 2
    near = n_fs - 1 - far
    reach = [(far, near) if p in (0, 2, 4, 6) else (near, far) for p in range(8)]

    def origin(d, h):
        return lax.rem(z + (n_fs - h if d == 0 else h), n_fs)

    def z_start(p, d, h):
        dev = {"fs": right_z if d == 0 else left_z}
        r = region(p, z if h == 1 else origin(d, h - 1), g)
        remote(r, r, z_send.at[p], z_recv.at[p, d, h - 1], dev).start()

    def z_event(p, d, h):
        dev = {"fs": left_z if d == 0 else right_z}
        arrive(region(p, origin(d, h), g), z_send.at[p], z_recv.at[p, d, h - 1], dev)

    def y_slot(p, h):
        return p if p < 3 else 2 + h

    def y_start(p, d, h):
        r = region(p, origin(d, h), g)
        remote(r, r, y_send.at[p], y_recv.at[y_slot(p, h)], {"grp": mate}).start()

    def y_done(p):
        arrive(whole(p), y_send.at[p], y_recv.at[p], {"grp": mate})

    def y_wait(h):
        pair = wdn.at[pl.ds(0, hd), pl.ds(0, (2 if h <= near else 1) * zd)]
        arrive(pair, y_send.at[3], y_recv.at[2 + h], {"grp": mate})

    steps = {RECV: z_event, Z_SEND: z_start, Y_SEND: y_start}
    order = ring_plan(reach, 4)
    done = [0]

    def take():
        _, kind, p, d, h = order[done[0]]
        steps[kind](p, d, h)
        done[0] += 1

    def pump_hop(pieces, h):
        need = {(p, d) for p in pieces for d in range(2) if h <= reach[p][d]}
        while any(o[1] == RECV and o[4] == h and o[2:4] in need for o in order[done[0] :]):
            take()

    def pump(until):
        while done[0] < len(order) and order[done[0]][0] <= until:
            take()

    def gather(i, view):
        ss = ag_send.at[i]
        rs = ag_recv.at[i]
        right, left, twin = {"tp": right_t}, {"tp": left_t}, {"tp": twin_t}

        def go(k, blk, half, dev):
            v = view(blk, half)
            send(v, v, ss, rs.at[min(k, 6)], dev)

        def got(k, blk, half, dev):
            arrive(view(blk, half), ss, rs.at[k], dev)

        def start():
            go(0, t, 0, right)
            go(2, t, 1, left)
            go(1, t, 1, right)
            go(3, t, 0, left)
            go(6, t, None, twin)

        def relay():
            got(0, left_t, 0, left)
            go(4, left_t, 0, right)
            got(2, right_t, 1, right)
            go(5, right_t, 1, left)

        def cross():
            got(1, left_t, 1, left)
            go(7, left_t, None, twin)
            got(3, right_t, 0, right)
            go(8, right_t, None, twin)

        def close():
            got(4, across_t, 0, left)
            go(9, across_t, 0, twin)
            got(5, across_t, 1, right)
            go(10, across_t, 1, twin)

        def finish():
            arrive(tok.at[:, pl.ds(0, n_x * cols)], ss, rs.at[6], twin)

        return start, relay, cross, close, finish

    def tok_view(blk, half):
        r = pl.ds(0, rows) if half is None else pl.ds(half * (rows // 2), rows // 2)
        return tok.at[r, pl.ds(at(blk, cols), cols)]

    def nrm_view(blk, half):
        cc = pl.ds(0, width) if half is None else pl.ds(half * (width // 2), width // 2)
        return nrm.at[pl.ds(at(blk, block), block), cc]

    rel = (2, 1, 0, 3)

    def scatter_sum(i, blk, bufs, cut, fill_twin, fill_own):
        ss = rs_send.at[i]
        rs = rs_recv.at[i]
        right, left, twin = {"tp": right_t}, {"tp": left_t}, {"tp": twin_t}
        pair_in, fwd_in, last_in, fwd_out, last_out = bufs
        for k in range(n_x):
            b = 2 * lax.rem(x + rel[k], n_x) + 1 - c
            fill_twin(b)
            send(blk(b), pair_in.at[k], ss, rs.at[k], twin)

        def pair(k):
            b = 2 * lax.rem(x + rel[k], n_x) + c
            fill_own(b)
            arrive(pair_in.at[k], ss, rs.at[k], twin)
            return blk(b)[...].astype(F32) + pair_in[k].astype(F32)

        def pass_on(src, dst, k, dev):
            send(src, dst, ss, rs.at[min(k, 6)], dev)

        s2 = pair(0)
        fwd_out[...] = s2.astype(BF)
        pass_on(cut(fwd_out, 0), fwd_in.at[0], 4, right)
        pass_on(cut(fwd_out, 1), fwd_in.at[1], 5, left)
        s1 = pair(1)
        last_out[0] = s1.astype(BF)
        pass_on(cut(last_out.at[0], 1), cut(last_in.at[0], 1), 6, right)
        s3 = pair(3)
        last_out[1] = s3.astype(BF)
        pass_on(cut(last_out.at[1], 0), cut(last_in.at[1], 0), 7, left)
        total = pair(2)
        yield
        arrive(fwd_in.at[0], ss, rs.at[4], left)
        head = cut(blk(2 * lax.rem(x + 1, n_x) + c), 0)[...].astype(F32)
        head = head + cut(pair_in.at[1], 0)[...].astype(F32) + fwd_in[0].astype(F32)
        cut(last_out.at[0], 0)[...] = head.astype(BF)
        pass_on(cut(last_out.at[0], 0), cut(last_in.at[0], 0), 8, right)
        arrive(fwd_in.at[1], ss, rs.at[5], right)
        head = cut(blk(2 * lax.rem(x + 3, n_x) + c), 1)[...].astype(F32)
        head = head + cut(pair_in.at[3], 1)[...].astype(F32) + fwd_in[1].astype(F32)
        cut(last_out.at[1], 1)[...] = head.astype(BF)
        pass_on(cut(last_out.at[1], 1), cut(last_in.at[1], 1), 9, left)
        yield
        arrive(last_in, ss, rs.at[6], left)
        yield total + last_in[0].astype(F32) + last_in[1].astype(F32)

    def row_block(b):
        return part1.at[pl.ds(at(b, block), block), :]

    def col_block(b):
        return part2.at[:, pl.ds(at(b, cols), cols)]

    def lane_half(ref, k):
        return ref.at[:, pl.ds(k * (width // 2), width // 2)]

    def row_half(ref, k):
        return ref.at[pl.ds(k * (rows // 2), rows // 2), :]

    def norm(v, gain):
        mean = jnp.mean(v, axis=1, keepdims=True)
        d = v - mean
        var = jnp.mean(d * d, axis=1, keepdims=True)
        return (d * lax.rsqrt(var + EPS) * gain).astype(BF)

    for i in (0, 1, 2, 3):
        moves[i].wait()
    tok_start, tok_relay, tok_cross, tok_close, tok_finish = gather(0, tok_view)
    pump(-0.5)
    for i in (4, 5, 6):
        moves[i].wait()
    pump(0.0)
    tok_start()
    mine = pl.ds(at(t, cols), cols)
    mg_all[:, mine] = m_gain[...]
    for k in range(1, n_tp):
        send(
            m_gain,
            mg_all.at[:, mine],
            small_send.at[0],
            small_recv.at[0],
            {"tp": lax.rem(t + k, n_tp)},
        )
    pump(5.5)
    tok_relay()
    pump(8.0)
    tok_cross()
    pump(10.8)
    tok_close()
    pump(12.0)
    tok_finish()

    key_cols = pl.ds(at(t, DK), DK)
    n_tiles = rows // TILE
    for i in range(7, 11):
        moves[i].wait()
    for i in range(n_tiles):
        rr = pl.ds(i * TILE, TILE)
        low = dot(tok[rr, :], fl[...], NT).astype(BF)
        pre = dot(low, d_up[...]) + d_bias[:, key_cols]
        log_sig = jnp.minimum(pre, 0.0) - jnp.log1p(jnp.exp(-jnp.abs(pre)))
        decay = log_sig / TAU + extra[rr, :]
        hi = decay.astype(BF)
        lo = (decay - hi.astype(F32)).astype(BF)
        esum[i] = jnp.exp(dot(sums[...], jnp.concatenate([hi, lo], axis=0)))
        pump(13.0 + i)
    pump(ATTEND)
    y_done(0)

    ii = lax.broadcasted_iota(jnp.int32, (TILE, TILE), 0)
    jj = lax.broadcasted_iota(jnp.int32, (TILE, TILE), 1)
    state = jnp.zeros((DV, DK), F32)
    n_lv = len(LEVELS)
    for i in range(n_tiles):
        rr = pl.ds(i * TILE, TILE)
        qkv = dot(tok[rr, :], wqkv[...]).astype(BF)
        q = qkv[:, :DK].astype(F32) * DK**-0.5
        kb = qkv[:, DK : 2 * DK]
        k = kb.astype(F32)
        v = qkv[:, 2 * DK :]
        scores = jnp.where(ii == jj, dot(q.astype(BF), kb, NT), 0.0)
        for l, m in enumerate(LEVELS):
            e = esum[i, pl.ds(l * TILE, TILE), :]
            s = dot((q * e).astype(BF), (k * e).astype(BF), NT)
            scores = jnp.where(((ii ^ jj) // m == 1) & (ii > jj), s, scores)
        e_in = esum[i, pl.ds(n_lv * TILE, TILE), :]
        e_out = esum[i, pl.ds((n_lv + 1) * TILE, TILE), :]
        got = dot(scores.astype(BF), v)
        if i > 0:
            got = got + dot((q * e_in).astype(BF), state.astype(BF), NT)
        if i < n_tiles - 1:
            fresh = dot(v, (k * e_out).astype(BF), TN)
            state = state * e_in[TILE - 1 : TILE, :] + fresh
        scale = lax.rsqrt(jnp.mean(got * got, axis=1, keepdims=True) + EPS)
        mixed[rr, :] = (got * scale * h_gain[...]).astype(BF)
        pump(ATTEND + 1.3 * i + 2.0)
    pump(ATTEND + 6.5)
    y_done(1)

    step = 256

    def mix_cols(j, _):
        cc = pl.ds(pl.multiple_of(j * step, step), step)
        part1[:, cc] = dot(mixed[...], wo[:, cc]).astype(BF)
        return 0

    lax.fori_loop(0, width // step, mix_cols, 0)
    pump(MIXED)

    def nothing(b):
        pass

    row_bufs = (pair_row, fwd_row_in, last_row_in, fwd_row_out, last_row_out)
    rs1 = scatter_sum(0, row_block, row_bufs, lane_half, nothing, nothing)
    next(rs1)
    pump(MIXED + 7.0)
    next(rs1)
    gains = mg_all.at[:, pl.ds(0, (n_tp - 1) * cols)]
    arrive(gains, small_send.at[0], small_recv.at[0], {"tp": twin_t})
    pump(MIXED + 11.5)
    mix = next(rs1)
    my_rows = pl.ds(at(t, block), block)
    nrm[my_rows, :] = norm(ALPHA * tok[my_rows, :].astype(F32) + mix, mg_all[...])
    n_start, n_relay, n_cross, n_close, n_finish = gather(1, nrm_view)
    n_start()
    pump(NORMED + 4.5)
    n_relay()
    pump(NORMED + 7.0)
    n_cross()
    pump(NORMED + 10.0)
    n_close()
    pump(NORMED + 11.0)
    n_finish()
    most = pl.ds(0, (n_tp - 1) * cols)
    for i in range(2):
        sent(tok.at[:, most], ag_send.at[i], ag_recv.at[i, 0])
    sent(tok.at[:, most], rs_send.at[0], rs_recv.at[0, 0])
    sent(gains, small_send.at[0], small_recv.at[0])
    pump(UP_READY)
    y_done(2)
    n_up = act.shape[1] // step

    def up_cols(j, _):
        cc = pl.ds(pl.multiple_of(j * step, step), step)
        hidden = jnp.maximum(dot(nrm[...], wup[:, cc]), 0.0)
        act[:, cc] = (hidden * hidden).astype(BF)
        return 0

    hops = [0]
    lax.fori_loop(0, n_up // 2, up_cols, 0)
    pump(UP_READY + 3.0)
    lax.fori_loop(n_up // 2, n_up, up_cols, 0)

    n_pairs = n_fs // 2
    for i, h in [(0, 1)] + [(k, min(2 * abs(k) + 1, far)) for m in range(1, far // 2) for k in (m, -m)] + [(far // 2, far)]:
        while hops[0] < h:
            hops[0] += 1
            pump_hop((3, 6, 7), hops[0])
            y_wait(hops[0])
        pump(DOWN + 1.2 * h)
        pair_at = lax.rem(z // 2 + i + n_pairs, n_pairs)
        cc = pl.ds(at(pair_at, 2 * zd), 2 * zd)
        part2[:, cc] = dot(act[...], wdn[:, cc]).astype(BF)
    pump(1e9)
    col_bufs = (pair_col, fwd_col_in, last_col_in, fwd_col_out, last_col_out)
    rs2 = scatter_sum(1, col_block, col_bufs, row_half, nothing, nothing)
    next(rs2)
    next(rs2)
    down = next(rs2)
    summed = ALPHA * nrm[:, mine].astype(F32) + down

    ones = jnp.ones((8, cols), BF)

    def row_sums(v):
        hi = v.astype(BF)
        lo = (v - hi.astype(F32)).astype(BF)
        return dot(ones, hi, NT) + dot(ones, lo, NT)

    stats[t, :, pl.ds(0, rows)] = row_sums(summed)[0:1, :]
    stats[t, :, pl.ds(rows, rows)] = row_sums(summed * summed)[0:1, :]
    for k in range(1, n_tp):
        send(
            stats.at[t],
            stats.at[t],
            small_send.at[1],
            small_recv.at[1],
            {"tp": lax.rem(t + k, n_tp)},
        )
    others = stats.at[pl.ds(0, n_tp - 1)]
    arrive(others, small_send.at[1], small_recv.at[1], {"tp": twin_t})
    both = stats[0]
    for k in range(1, n_tp):
        both = both + stats[k]
    first = lax.broadcasted_iota(jnp.int32, (8, rows), 0) == 0
    both = jnp.transpose(jnp.where(first, both[:, :rows], both[:, rows:])) / width
    mean, square = both[:, 0:1], both[:, 1:2]
    scale = lax.rsqrt(square - mean * mean + EPS)
    out[...] = ((summed - mean) * scale * o_gain[...]).astype(BF)
    sent(tok.at[:, most], rs_send.at[1], rs_recv.at[1, 0])
    sent(others, small_send.at[1], small_recv.at[1])
    for p in range(8):
        w = whole(p)
        remote(w, w, z_send.at[p], z_recv.at[p, 0, 0], {"fs": right_z}).wait_send()
        if p < 4:
            remote(w, w, y_send.at[p], y_recv.at[p], {"grp": mate}).wait_send()


def solution(mesh):
    n_fs, n_tp = mesh.shape["fs"], mesh.shape["tp"]
    assert n_tp == 8 and mesh.shape["grp"] % 2 == 0

    def local(
        tokens,
        query_matrix,
        key_weight,
        value_weight,
        forget_lower_factor,
        decay_up,
        decay_bias,
        log_extra,
        head_gain,
        out_weight,
        mix_gain,
        up_weight,
        down_weight,
        out_gain,
    ):
        rows, cols = tokens.shape
        width = cols * n_tp
        block = rows // n_tp
        zd = query_matrix.shape[0]
        hidden = up_weight.shape[1]
        vcols = value_weight.shape[1]
        qkv_cols = 2 * query_matrix.shape[1] + vcols
        sums = jnp.asarray(decay_sums(), BF)
        hbm = pl.BlockSpec(memory_space=pl.ANY)
        vmem = pl.BlockSpec(memory_space=pltpu.VMEM)
        far = n_fs // 2
        dma = pltpu.SemaphoreType.DMA
        return pl.pallas_call(
            functools.partial(kernel, n_fs, n_tp),
            out_shape=jax.ShapeDtypeStruct((rows, cols), BF),
            in_specs=[hbm] * 11 + [vmem] * 4,
            out_specs=vmem,
            scratch_shapes=[
                pltpu.VMEM((rows, width), BF),
                pltpu.VMEM((width, qkv_cols), BF),
                pltpu.VMEM((vcols, width), BF),
                pltpu.VMEM((width, hidden), BF),
                pltpu.VMEM((hidden, width), BF),
                pltpu.VMEM((rows // TILE, sums.shape[0], DK), F32),
                pltpu.VMEM((rows, vcols), BF),
                pltpu.VMEM((rows, width), BF),
                pltpu.VMEM((rows, width), BF),
                pltpu.VMEM((n_tp // 2, block, width), BF),
                pltpu.VMEM((2, block, width // 2), BF),
                pltpu.VMEM((2, block, width), BF),
                pltpu.VMEM((block, width), BF),
                pltpu.VMEM((2, block, width), BF),
                pltpu.VMEM((n_tp // 2, rows, cols), BF),
                pltpu.VMEM((2, rows // 2, cols), BF),
                pltpu.VMEM((2, rows, cols), BF),
                pltpu.VMEM((rows, cols), BF),
                pltpu.VMEM((2, rows, cols), BF),
                pltpu.VMEM((rows, width), BF),
                pltpu.VMEM((rows, hidden), BF),
                pltpu.VMEM((n_tp, 1, 2 * rows), F32),
                pltpu.VMEM((1, width), F32),
                pltpu.VMEM(forget_lower_factor.shape[::-1], BF),
                pltpu.VMEM((decay_up.shape[0], DK), BF),
                pltpu.VMEM(log_extra.shape, F32),
                pltpu.VMEM(sums.shape, BF),
                dma((11,)),
                dma((8,)),
                dma((8, 2, far)),
                dma((4,)),
                dma((3 + far,)),
                dma((2,)),
                dma((2, 7)),
                dma((2,)),
                dma((2, 7)),
                dma((2,)),
                dma((2,)),
            ],
            compiler_params=pltpu.CompilerParams(
                collective_id=0,
                has_side_effects=True,
                vmem_limit_bytes=60 * 1024 * 1024,
            ),
            name="layer",
        )(
            tokens,
            query_matrix,
            key_weight,
            value_weight,
            out_weight,
            up_weight,
            down_weight,
            forget_lower_factor.T,
            decay_up,
            log_extra,
            sums,
            decay_bias.reshape(1, -1),
            head_gain.reshape(1, -1),
            mix_gain.reshape(1, -1),
            out_gain.reshape(1, -1),
        )

    in_specs = (
        P(("grp", "fs"), "tp"),
        P("fs", "tp"),
        P("fs", "tp"),
        P("fs", "tp"),
        P(),
        P(),
        P(),
        P(("grp", "fs"), "tp"),
        P(),
        P("tp", "fs"),
        P("tp"),
        P("fs", "tp"),
        P("tp", "fs"),
        P("tp"),
    )
    out_specs = P(("grp", "fs"), "tp")
    return jax.shard_map(local, mesh=mesh, in_specs=in_specs, out_specs=out_specs, check_vma=False)
```
